32 devices in a mesh: fs: 8 (over z, x), tp: 4 (over y, core).
Axes of the slice: x: 2, y: 2, z: 4, core: 2. Of those that a mesh axis runs over, the one named last changes fastest.
Arguments:
- mixer_input: bfloat16 [8192, 4096], P('fs'), may hold values from -6 to 6
- cell_output: bfloat16 [8192, 2048], P('fs'), may hold values from -6 to 6
- query_grad: bfloat16 [8192, 2048], P('fs', 'tp'), may hold values from -4 to 4
- value_grad: bfloat16 [8192, 2048], P('fs', 'tp'), may hold values from -4 to 4
- output_grad: bfloat16 [8192, 4096], P('fs', 'tp'), may hold values from -4 to 4
- query_weight: float32 [4096, 2048], P('fs', 'tp'), may hold values from -6 to 6
- value_weight: float32 [4096, 2048], P('fs', 'tp'), may hold values from -6 to 6
- output_weight: float32 [2048, 4096], P('fs', 'tp'), may hold values from -6 to 6
- query_basis: bfloat16 [4096, 128], P('fs'), may hold values from -0.09375 to 0.09375
- value_basis: bfloat16 [4096, 128], P('fs'), may hold values from -0.09375 to 0.09375
- output_basis: bfloat16 [2048, 128], P('fs'), may hold values from -0.125 to 0.125
- query_mean: float32 [128, 2048], P(None, 'tp'), may hold values from -6 to 6
- value_mean: float32 [128, 2048], P(None, 'tp'), may hold values from -6 to 6
- output_mean: float32 [128, 4096], P(None, 'tp'), may hold values from -6 to 6
- query_square: float32 [128, 2048], P(None, 'tp'), may hold values from 0.25 to 4
- value_square: float32 [128, 2048], P(None, 'tp'), may hold values from 0.25 to 4
- output_square: float32 [128, 4096], P(None, 'tp'), may hold values from 0.25 to 4
Outputs:
- query_step: float32 [4096, 2048], P('fs', 'tp')
- value_step: float32 [4096, 2048], P('fs', 'tp')
- output_step: float32 [2048, 4096], P('fs', 'tp')
- query_copy: bfloat16 [4096, 2048], P(None, 'tp')
- value_copy: bfloat16 [4096, 2048], P(None, 'tp')
- output_copy: bfloat16 [2048, 4096], P(None, 'tp')
- query_first: float32 [128, 2048], P(None, 'tp')
- value_first: float32 [128, 2048], P(None, 'tp')
- output_first: float32 [128, 4096], P(None, 'tp')
- query_second: float32 [128, 2048], P(None, 'tp')
- value_second: float32 [128, 2048], P(None, 'tp')
- output_second: float32 [128, 4096], P(None, 'tp')
The draws below stay inside these ranges and needn't reach their ends.
All inputs are finite; a program needn't handle non-finite values.
Results may differ from the reference program's by a relative error of at most 0.013.
Values may be sent and summed in bfloat16 or wider, within the bound.
A program may use at most 128 MiB of HBM per device.

```python
import math
import jax
import jax.numpy as jnp
from jax import lax

MODEL = 4096
CELL = 2048
RANK = 128
TOKENS = 8192


def input_rows(key):
    return jnp.clip(jax.random.normal(jax.random.fold_in(key, 101), (TOKENS, MODEL), jnp.float32), -6.0, 6.0)


def readout_rows(key):
    return jnp.clip(jax.random.normal(jax.random.fold_in(key, 102), (TOKENS, CELL), jnp.float32), -6.0, 6.0)


def coherent_grad(key, rows, salt, width):
    inner = rows.shape[1]
    noise = jnp.clip(jax.random.normal(jax.random.fold_in(key, salt), (TOKENS, width), jnp.float32), -6.0, 6.0) * (1.0 / math.sqrt(TOKENS))
    heading = jax.random.normal(jax.random.fold_in(key, salt + 1), (inner,), jnp.float32) * (1.0 / math.sqrt(inner))
    column = jnp.clip(jax.random.normal(jax.random.fold_in(key, salt + 2), (width,), jnp.float32), -3.0, 3.0)
    strength = 4.0 * math.sqrt(inner) / TOKENS
    along = jnp.dot(rows, heading, precision=lax.Precision.HIGHEST)
    return jnp.clip(noise + strength * along[:, None] * column[None, :], -4.0, 4.0)


def draw_mixer_input(key, part):
    return input_rows(key).astype(jnp.bfloat16)


def draw_cell_output(key, part):
    return readout_rows(key).astype(jnp.bfloat16)


def draw_query_grad(key, part):
    return coherent_grad(key, input_rows(key), 201, CELL).astype(jnp.bfloat16)


def draw_value_grad(key, part):
    return coherent_grad(key, input_rows(key), 211, CELL).astype(jnp.bfloat16)


def draw_output_grad(key, part):
    return coherent_grad(key, readout_rows(key), 221, MODEL).astype(jnp.bfloat16)


def shard_levels(key, dims, pieces, low, high):
    level, own = 1.0, jax.random.fold_in(key, 6)
    for axis_at, blocks in pieces:
        heights = jnp.exp(jax.random.uniform(jax.random.fold_in(own, axis_at), (blocks,), jnp.float32, low / len(pieces), high / len(pieces)))
        level = level * jnp.repeat(heights, dims[axis_at] // blocks).reshape([-1 if axis == axis_at else 1 for axis in range(len(dims))])
    return level


def gaussian(own_key, extent, deviation, reach, cuts=(), kind=jnp.bfloat16):
    array = deviation * jax.random.normal(own_key, extent, jnp.float32)
    if cuts:
        array = array * shard_levels(own_key, extent, cuts, -0.22, 0.18)
    return jnp.clip(array, -reach, reach).astype(kind)


def setup_inputs(seed: int = 0) -> dict:
    seeds = jax.random.split(jax.random.key(seed), 18)
    return {
        "mixer_input": draw_mixer_input(jax.random.fold_in(seeds[17], 71), 0),
        "cell_output": draw_cell_output(jax.random.fold_in(seeds[17], 71), 0),
        "query_grad": draw_query_grad(jax.random.fold_in(seeds[17], 71), 0),
        "value_grad": draw_value_grad(jax.random.fold_in(seeds[17], 71), 0),
        "output_grad": draw_output_grad(jax.random.fold_in(seeds[17], 71), 0),
        "query_weight": gaussian(seeds[5], (MODEL, CELL), 1.0, 6.0, ((0, 8), (1, 4)), jnp.float32),
        "value_weight": gaussian(seeds[6], (MODEL, CELL), 1.0, 6.0, ((0, 8), (1, 4)), jnp.float32),
        "output_weight": gaussian(seeds[7], (CELL, MODEL), 1.0, 6.0, ((0, 8), (1, 4)), jnp.float32),
        "query_basis": gaussian(seeds[8], (MODEL, RANK), MODEL ** -0.5, 0.09375, ((0, 8),)),
        "value_basis": gaussian(seeds[9], (MODEL, RANK), MODEL ** -0.5, 0.09375, ((0, 8),)),
        "output_basis": gaussian(seeds[10], (CELL, RANK), CELL ** -0.5, 0.125, ((0, 8),)),
        "query_mean": gaussian(seeds[11], (RANK, CELL), 1.0, 6.0, ((1, 4),), jnp.float32),
        "value_mean": gaussian(seeds[12], (RANK, CELL), 1.0, 6.0, ((1, 4),), jnp.float32),
        "output_mean": gaussian(seeds[13], (RANK, MODEL), 1.0, 6.0, ((1, 4),), jnp.float32),
        "query_square": jnp.clip(jnp.exp(math.log(4.0) - 2.7725887 * jax.random.uniform(seeds[14], (RANK, CELL), jnp.float32) ** shard_levels(seeds[14], (RANK, CELL), ((1, 4),), -0.2, 0.2)), 0.25, 4.0),
        "value_square": jnp.clip(jnp.exp(math.log(4.0) - 2.7725887 * jax.random.uniform(seeds[15], (RANK, CELL), jnp.float32) ** shard_levels(seeds[15], (RANK, CELL), ((1, 4),), -0.2, 0.2)), 0.25, 4.0),
        "output_square": jnp.clip(jnp.exp(math.log(4.0) - 2.7725887 * jax.random.uniform(seeds[16], (RANK, MODEL), jnp.float32) ** shard_levels(seeds[16], (RANK, MODEL), ((1, 4),), -0.2, 0.2)), 0.25, 4.0),
    }


beta_first = 0.8
beta_second = 0.9
floor_mean = 0.005
learn_rate = 0.05

def across(leading, trailing):
    return lax.dot_general(leading, trailing, (((0,), (0,)), ((), ())), preferred_element_type=jnp.float32)

def moments(gradient, basis, mean_old, square_old):
    factor_full = basis.astype(jnp.float32)
    projected = lax.dot_general(factor_full, gradient, (((0,), (0,)), ((), ())), precision=lax.Precision.HIGHEST, preferred_element_type=jnp.float32)
    moment_one = beta_first * mean_old + (1.0 - beta_first) * projected
    moment_two = beta_second * square_old + (1.0 - beta_second) * projected * projected
    direction = moment_one / jnp.sqrt(moment_two)
    lowrank = jnp.dot(factor_full, direction, precision=lax.Precision.HIGHEST, preferred_element_type=jnp.float32)
    return (lowrank, moment_one, moment_two)

def reference(mixer_input, cell_output, query_grad, value_grad, output_grad, query_weight, value_weight, output_weight, query_basis, value_basis, output_basis, query_mean, value_mean, output_mean, query_square, value_square, output_square):
    gradient_query = across(mixer_input, query_grad)
    gradient_value = across(mixer_input, value_grad)
    gradient_output = across(cell_output, output_grad)
    low_query, query_first, query_second = moments(gradient_query, query_basis, query_mean, query_square)
    low_value, value_first, value_second = moments(gradient_value, value_basis, value_mean, value_square)
    low_output, output_first, output_second = moments(gradient_output, output_basis, output_mean, output_square)
    squares = jnp.sum(low_query * low_query) + jnp.sum(low_value * low_value) + jnp.sum(low_output * low_output)
    factor = 1.0 / jnp.sqrt(squares / (3.0 * MODEL * CELL) + floor_mean)
    query_step = -factor * low_query
    value_step = -factor * low_value
    output_step = -factor * low_output
    query_copy = (query_weight + learn_rate * query_step).astype(jnp.bfloat16)
    value_copy = (value_weight + learn_rate * value_step).astype(jnp.bfloat16)
    output_copy = (output_weight + learn_rate * output_step).astype(jnp.bfloat16)
    return (query_step, value_step, output_step, query_copy, value_copy, output_copy, query_first, value_first, output_first, query_second, value_second, output_second)
```

```python
import functools

import jax
import jax.numpy as jnp
from jax import lax
from jax.experimental import pallas as pl
from jax.experimental.pallas import tpu as pltpu
from jax.sharding import PartitionSpec as P

beta_first = 0.8
beta_second = 0.9
floor_mean = 0.005
learn_rate = 0.05

MESH = pl.DeviceIdType.MESH
LINE_CHUNKS = 5
CHUNKS = 4


def matmul(left, right):
    return jnp.dot(left, right, preferred_element_type=jnp.float32)


def moments(projected, mean_old, square_old):
    moment_one = beta_first * mean_old + (1.0 - beta_first) * projected
    moment_two = beta_second * square_old + (1.0 - beta_second) * projected * projected
    return (moment_one, moment_two, moment_one / jnp.sqrt(moment_two))


def aligned(start, size):
    return pl.ds(pl.multiple_of(start, size), size)


class Weights:
    def __init__(self, wholes, fs, me, send_sem, recv_sem):
        self.wholes, self.fs, self.me = wholes, fs, me
        self.send_sem, self.recv_sem = send_sem, recv_sem
        self.relayed = fs == 8
        self.place, self.side = me // 2, lax.rem(me, 2)

    def index(self, step, other=False):
        place = lax.rem(self.place + step + 4, 4)
        return place * 2 + (1 - self.side if other else self.side)

    def slot(self, w, i, origin):
        whole = self.wholes[w]
        block = whole.shape[0] // self.fs
        rows = block // CHUNKS
        return whole.at[aligned(origin * block + i * rows, rows), :]

    def copy(self, w, i, origin, site, role, target):
        return pltpu.make_async_remote_copy(
            src_ref=self.slot(w, i, origin),
            dst_ref=self.slot(w, i, origin),
            send_sem=self.send_sem.at[w, i, site],
            recv_sem=self.recv_sem.at[w, i, role],
            device_id={"fs": target},
            device_id_type=MESH,
        )

    def arrive(self, w, i, origin, role, inside):
        copy = self.copy(w, i, origin, 0, role, lax.rem(self.me + 1, self.fs))
        if inside is True:
            copy.wait_recv()
        else:
            pl.when(inside)(copy.wait_recv)

    def sites(self, w, i):
        p = self.place
        line = i * len(self.wholes) + w < LINE_CHUNKS
        out = [
            (0, self.me, 0, self.index(1), p < 3),
            (1, self.me, 3, self.index(-1), p > 0),
            (2, self.me, 6, self.index(0, True), True),
        ]
        cross = self.index(0, True)
        for d in (1, 2):
            out.append((2 + d, self.index(-d), d, self.index(1), (p >= d) & (p < 3)))
            out.append((4 + d, self.index(d), 3 + d, self.index(-1), (p + d < 4) & (p > 0)))
        for d in (1, 2, 3):
            below, above = p >= d, p + d < 4
            if d == 1:
                below = below & jnp.logical_not(line | (p == 1))
                above = above & jnp.logical_not(line | (p == 2))
            out.append((6 + d, self.index(-d), 6 + d, cross, below))
            out.append((9 + d, self.index(d), 9 + d, cross, above))
        out.append((13, cross, 7, self.index(1), (p < 3) & (line | (p == 0))))
        out.append((14, cross, 10, self.index(-1), (p > 0) & (line | (p == 3))))
        return {site[0]: site for site in out}

    def direct(self, w, i):
        return {
            k - 1: (k - 1, self.me, k - 1, lax.rem(self.me + k, self.fs), True)
            for k in range(1, self.fs)
        }

    def send(self, w, i, *wanted):
        table = self.sites(w, i)
        for site in wanted:
            number, origin, role, target, inside = table[site]
            copy = self.copy(w, i, origin, number, role, target)
            if inside is True:
                copy.start()
            else:
                pl.when(inside)(copy.start)

    def each(self, step):
        def chunk(i, carry):
            for w in range(len(self.wholes)):
                step(w, i)
            return carry

        lax.fori_loop(0, CHUNKS, chunk, 0)

    def start(self):
        def step(w, i):
            if self.relayed:
                self.send(w, i, 0, 1, 2)
            else:
                for number, origin, role, target, _ in self.direct(w, i).values():
                    self.copy(w, i, origin, number, role, target).start()

        self.each(step)

    def relay(self, d):
        if not self.relayed:
            return
        p = self.place

        def step(w, i):
            self.arrive(w, i, self.index(-d), d - 1, p >= d)
            self.send(w, i, *((2 + d, 6 + d) if d < 3 else (6 + d,)))
            self.arrive(w, i, self.index(d), 2 + d, p + d < 4)
            self.send(w, i, *((4 + d, 9 + d) if d < 3 else (9 + d,)))

        self.each(step)

    def relay_cross(self):
        if not self.relayed:
            return

        def step(w, i):
            self.arrive(w, i, self.index(0, True), 6, True)
            self.send(w, i, 13, 14)

        self.each(step)

    def finish(self):
        p = self.place

        def step(w, i):
            if not self.relayed:
                for k in range(1, self.fs):
                    self.arrive(w, i, lax.rem(self.me + self.fs - k, self.fs), k - 1, True)
                for number, origin, role, target, _ in self.direct(w, i).values():
                    self.copy(w, i, origin, number, role, target).wait_send()
                return
            for d in (1, 2, 3):
                self.arrive(w, i, self.index(-d, True), 6 + d, p >= d)
                self.arrive(w, i, self.index(d, True), 9 + d, p + d < 4)
            for number, origin, role, target, inside in self.sites(w, i).values():
                copy = self.copy(w, i, origin, number, role, target)
                if inside is True:
                    copy.wait_send()
                else:
                    pl.when(inside)(copy.wait_send)

        self.each(step)


def remote(ref_from, ref_to, send, recv, **device):
    return pltpu.make_async_remote_copy(
        src_ref=ref_from,
        dst_ref=ref_to,
        send_sem=send,
        recv_sem=recv,
        device_id=device,
        device_id_type=MESH,
    )


def kernel(
    fs,
    tp,
    owners,
    mixer_hbm,
    cell_hbm,
    qg_hbm,
    vg_hbm,
    og_hbm,
    qb_hbm,
    vb_hbm,
    ob_hbm,
    qw_hbm,
    vw_hbm,
    ow_hbm,
    qm,
    vm,
    om,
    qs,
    vs,
    os,
    qw_all,
    vw_all,
    ow_all,
    pair_all,
    ob_all,
    proj,
    squares,
    mixer,
    cell,
    qg,
    vg,
    og,
    qw,
    vw,
    ow,
    part,
    parts,
    square_own,
    square_in,
    w_send,
    w_recv,
    b_send,
    b_recv,
    y_send,
    y_recv,
    c_send,
    c_recv,
    sum_send,
    sum_recv,
    back_send,
    back_recv,
    tp_send,
    tp_recv,
    local_sem,
):
    me, column = lax.axis_index("fs"), lax.axis_index("tp")
    rank, width = qm.shape
    far, core = column // 2, lax.rem(column, 2)
    fars = tp // 2
    own_bases = (pair_all.at[me, far, core], ob_all.at[me, far, core])
    pair_rows, ob_rows = pair_all.shape[3], ob_all.shape[3]
    pair_from = aligned(column * pair_rows, pair_rows)
    ob_from = aligned(column * ob_rows, ob_rows)
    loads = [
        pltpu.make_async_copy(source, target, local_sem.at[i])
        for i, (source, target) in enumerate(
            (
                (qb_hbm.at[pair_from, :], pair_all.at[me, far, core, :, pl.ds(0, rank)]),
                (vb_hbm.at[pair_from, :], pair_all.at[me, far, core, :, pl.ds(rank, rank)]),
                (ob_hbm.at[ob_from, :], own_bases[1]),
                (qw_hbm, qw),
                (vw_hbm, vw),
                (ow_hbm, ow),
                (mixer_hbm, mixer),
                (cell_hbm, cell),
                (qg_hbm, qg),
                (vg_hbm, vg),
                (og_hbm, og),
            )
        )
    ]
    for load in loads:
        load.start()

    barrier = pltpu.get_barrier_semaphore()
    for k in range(1, fs):
        pl.semaphore_signal(
            barrier, inc=1, device_id={"fs": lax.rem(me + k, fs)}, device_id_type=MESH
        )
    for k in range(1, tp):
        pl.semaphore_signal(
            barrier, inc=1, device_id={"tp": lax.rem(column + k, tp)}, device_id_type=MESH
        )
    pl.semaphore_wait(barrier, fs + tp - 2)

    for load in loads[:3]:
        load.wait()
    bases = (pair_all, ob_all)
    sent = []
    for k in range(1, fs):
        for n, whole in enumerate(bases):
            mine = whole.at[me, far, core]
            copy = remote(
                mine,
                mine,
                b_send.at[n, k - 1],
                b_recv.at[n, k - 1],
                fs=lax.rem(me + k, fs),
            )
            copy.start()
            sent.append(copy)

    for load in loads[3:6]:
        load.wait()
    wholes = (qw_all, vw_all, ow_all)
    for own, whole in zip((qw, vw, ow), wholes):
        block = own.shape[0]
        whole[aligned(me * block, block), :] = own[...].astype(jnp.bfloat16)
    weights = Weights(wholes, fs, me, w_send, w_recv)
    weights.start()
    part[...] = jnp.zeros_like(part)

    for k in range(1, fs):
        source = lax.rem(me + fs - k, fs)
        for n, whole in enumerate(bases):
            there = whole.at[source, far, core]
            remote(
                there,
                there,
                b_send.at[n, k - 1],
                b_recv.at[n, k - 1],
                fs=lax.rem(me + k, fs),
            ).wait_recv()
    for k in range(1, fars):
        for n, whole in enumerate(bases):
            mine = whole.at[:, far, core]
            copy = remote(
                mine,
                mine,
                y_send.at[n, k - 1],
                y_recv.at[n, k - 1],
                tp=lax.rem(far + k, fars) * 2 + core,
            )
            copy.start()
            sent.append(copy)
    for k in range(1, fars):
        source = lax.rem(far + fars - k, fars)
        for n, whole in enumerate(bases):
            there = whole.at[:, source, core]
            remote(
                there,
                there,
                y_send.at[n, k - 1],
                y_recv.at[n, k - 1],
                tp=lax.rem(far + k, fars) * 2 + core,
            ).wait_recv()
    for n, whole in enumerate(bases):
        mine = whole.at[:, :, core]
        copy = remote(mine, mine, c_send.at[n], c_recv.at[n], tp=far * 2 + 1 - core)
        copy.start()
        sent.append(copy)
    for load in loads[6:]:
        load.wait()
    for n, whole in enumerate(bases):
        there = whole.at[:, :, 1 - core]
        remote(there, there, c_send.at[n], c_recv.at[n], tp=far * 2 + 1 - core).wait_recv()

    tile = 256

    def project(rows, grad):
        turned = jnp.transpose(rows)
        high = turned.astype(jnp.bfloat16)
        low = (turned - high.astype(jnp.float32)).astype(jnp.bfloat16)
        both = matmul(jnp.concatenate([high, low], axis=0), grad)
        return both[:rank] + both[rank:]

    def flat(ref):
        value = ref[...]
        return value.reshape(-1, value.shape[-1])

    def step(t, carry):
        at = aligned(t * tile, tile)
        rows = matmul(mixer[at, :], flat(pair_all))
        part[:, :width] += project(rows[:, :rank], qg[at, :])
        part[:, width : 2 * width] += project(rows[:, rank:], vg[at, :])
        part[:, 2 * width :] += project(matmul(cell[at, :], flat(ob_all)), og[at, :])
        return carry

    lax.fori_loop(0, mixer.shape[0] // tile, step, 0)

    first_owner = (fs - owners) // 2
    share = rank // owners

    def owns(index):
        return (index >= first_owner) & (index < first_owner + owners)

    def strip_of(index):
        return lax.rem(index - first_owner + fs, owners)

    def strip(index):
        return aligned(strip_of(index) * share, share)

    drains = []
    for k in range(1, fs):
        target = lax.rem(me + k, fs)
        copy = remote(
            part.at[strip(target), :],
            parts.at[k - 1],
            sum_send.at[k - 1],
            sum_recv.at[k - 1],
            fs=target,
        )
        pl.when(owns(target))(copy.start)
        drains.append((copy, owns(target)))

    weights.relay(1)

    def gram(ref):
        rows, size = ref.shape[3], ref.shape[4]

        def add(i, total):
            piece = ref[i].reshape(-1, size)
            turned = jnp.transpose(piece.astype(jnp.float32)).astype(jnp.bfloat16)
            return total + matmul(turned, piece)

        return lax.fori_loop(0, ref.shape[0], add, jnp.zeros((size, size), jnp.float32))

    gram_pair = gram(pair_all)
    gram_output = gram(ob_all)

    back = []
    for k in range(1, fs):
        target = lax.rem(me + k, fs)
        mine = proj.at[strip(me), :]
        back.append(
            remote(mine, mine, back_send.at[k - 1], back_recv.at[k - 1], fs=target)
        )

    @pl.when(owns(me))
    def _():
        for k in range(1, fs):
            remote(
                part.at[strip(me), :],
                parts.at[k - 1],
                sum_send.at[k - 1],
                sum_recv.at[k - 1],
                fs=lax.rem(me + k, fs),
            ).wait_recv()
        total = part[strip(me), :]
        for k in range(1, fs):
            total = total + parts[k - 1]
        proj[strip(me), :] = total.astype(proj.dtype)
        for copy in back:
            copy.start()

    weights.relay(2)
    weights.relay_cross()

    for k in range(1, fs):
        source = lax.rem(me + fs - k, fs)
        there = proj.at[strip(source), :]
        copy = remote(
            there, there, back_send.at[k - 1], back_recv.at[k - 1], fs=lax.rem(me + k, fs)
        )
        pl.when(owns(source))(copy.wait_recv)

    def norm(basis_gram, projected, mean, square):
        direction = moments(projected.astype(jnp.float32), mean[...], square[...])[2]
        turned = jnp.dot(
            basis_gram,
            direction,
            precision=lax.Precision.HIGHEST,
            preferred_element_type=jnp.float32,
        )
        lanes = jnp.sum(direction * turned, axis=0, keepdims=True)
        return jnp.sum(lanes, axis=1, keepdims=True)

    partial = (
        norm(gram_pair[:rank, :rank], proj[:, :width], qm, qs)
        + norm(gram_pair[rank:, rank:], proj[:, width : 2 * width], vm, vs)
        + norm(gram_output, proj[:, 2 * width :], om, os)
    )
    square_own[...] = jnp.broadcast_to(partial, square_own.shape)
    shares = []
    for k in range(1, tp):
        copy = remote(
            square_own,
            square_in.at[k - 1],
            tp_send.at[k - 1],
            tp_recv.at[k - 1],
            tp=lax.rem(column + k, tp),
        )
        copy.start()
        shares.append(copy)

    weights.relay(3)
    for copy in shares:
        copy.wait_recv()
    whole_squares = square_own[...]
    for k in range(1, tp):
        whole_squares = whole_squares + square_in[k - 1]
    squares[...] = whole_squares
    weights.finish()
    for copy in sent + shares:
        copy.wait_send()
    for copy, inside in drains:
        pl.when(inside)(copy.wait_send)

    @pl.when(owns(me))
    def _():
        for copy in back:
            copy.wait_send()


def exchange(fs, tp, mixer, cell, grads, bases, weights, means, olds):
    rank = means[0].shape[0]
    total = sum(grad.shape[1] for grad in grads)
    owners = min(4, fs)
    bf16, f32 = jnp.bfloat16, jnp.float32
    hbm, vmem = pl.BlockSpec(memory_space=pl.ANY), pl.BlockSpec(memory_space=pltpu.VMEM)
    dma = pltpu.SemaphoreType.DMA

    def whole(array):
        return jax.ShapeDtypeStruct((array.shape[0] * fs, array.shape[1]), bf16)

    def parted(array, columns):
        return jax.ShapeDtypeStruct((fs, tp // 2, 2, array.shape[0] // tp, columns), bf16)

    return pl.pallas_call(
        functools.partial(kernel, fs, tp, owners),
        out_shape=(
            *(whole(weight) for weight in weights),
            parted(bases[0], 2 * rank),
            parted(bases[2], rank),
            jax.ShapeDtypeStruct((rank, total), bf16),
            jax.ShapeDtypeStruct((8, 128), f32),
        ),
        in_specs=[hbm] * 11 + [vmem] * 6,
        out_specs=(vmem,) * 7,
        scratch_shapes=[
            *(pltpu.VMEM(array.shape, bf16) for array in (mixer, cell, *grads)),
            *(pltpu.VMEM(array.shape, f32) for array in weights),
            pltpu.VMEM((rank, total), f32),
            pltpu.VMEM((fs - 1, rank // owners, total), f32),
            pltpu.VMEM((8, 128), f32),
            pltpu.VMEM((tp - 1, 8, 128), f32),
            dma((3, CHUNKS, max(15, fs - 1))),
            dma((3, CHUNKS, max(13, fs - 1))),
            dma((2, fs - 1)),
            dma((2, fs - 1)),
            dma((2, max(1, tp // 2 - 1))),
            dma((2, max(1, tp // 2 - 1))),
            dma((2,)),
            dma((2,)),
            dma((fs - 1,)),
            dma((fs - 1,)),
            dma((fs - 1,)),
            dma((fs - 1,)),
            dma((tp - 1,)),
            dma((tp - 1,)),
            dma((11,)),
        ],
        compiler_params=pltpu.CompilerParams(
            collective_id=0, has_side_effects=True, vmem_limit_bytes=VMEM_MAIN
        ),
    )(mixer, cell, *grads, *bases, *weights, *means, *olds)


VMEM_MAIN = 28 * 1024 * 1024
VMEM_LAST = 24 * 1024 * 1024


def last_kernel(entries, *refs):
    inputs, outputs, scratch = refs[:13], refs[13:25], refs[25:]
    wholes, pair, ob, proj, squares = inputs[0:3], inputs[3], inputs[4], inputs[5], inputs[6]
    means, olds = inputs[7:10], inputs[10:13]
    stage, sem = scratch[:12], scratch[12]
    rank, width = means[0].shape
    me = lax.axis_index("fs")
    factor = 1.0 / jnp.sqrt(squares[0:1, 0:1] / entries + floor_mean)
    copies = []

    def put(index, source, target):
        copy = pltpu.make_async_copy(source, target, sem.at[len(copies)])
        copy.start()
        copies.append(copy)

    bases = ((pair, 0), (pair, rank), (ob, 0))
    lefts = (0, width, 2 * width)
    for n in range(3):
        columns = means[n].shape[1]
        projected = proj[:, lefts[n] : lefts[n] + columns].astype(jnp.float32)
        first, second, direction = moments(projected, means[n][...], olds[n][...])
        stage[6 + n][...] = first
        stage[9 + n][...] = second
        put(6 + n, stage[6 + n], outputs[6 + n])
        put(9 + n, stage[9 + n], outputs[9 + n])
        high = direction.astype(jnp.bfloat16)
        low = (direction - high.astype(jnp.float32)).astype(jnp.bfloat16)
        both = jnp.concatenate([high, low], axis=0)
        base, left = bases[n]
        blocks = wholes[n].shape[0] // base.shape[0]
        own = base[me, :, left : left + rank]
        stage[n][...] = -factor * matmul(jnp.concatenate([own, own], axis=1), both)
        put(n, stage[n], outputs[n])
        scale = (-learn_rate) * factor
        for o in range(base.shape[0]):
            rows = pl.ds(o * blocks, blocks)
            piece = base[o, :, left : left + rank]
            update = matmul(piece, high)
            stage[3 + n][rows, :] = (
                wholes[n][rows, :].astype(jnp.float32) + scale * update
            ).astype(jnp.bfloat16)
            put(3 + n, stage[3 + n].at[rows, :], outputs[3 + n].at[rows, :])
    for copy in copies:
        copy.wait()


def body(fs, tp):
    def local(
        mixer_input,
        cell_output,
        query_grad,
        value_grad,
        output_grad,
        query_weight,
        value_weight,
        output_weight,
        query_basis,
        value_basis,
        output_basis,
        query_mean,
        value_mean,
        output_mean,
        query_square,
        value_square,
        output_square,
    ):
        means = (query_mean, value_mean, output_mean)
        olds = (query_square, value_square, output_square)
        weights = (query_weight, value_weight, output_weight)
        *wholes, pair, ob, proj, squares = exchange(
            fs,
            tp,
            mixer_input,
            cell_output,
            (query_grad, value_grad, output_grad),
            (query_basis, value_basis, output_basis),
            weights,
            means,
            olds,
        )
        entries = float(sum(w.shape[0] * fs * w.shape[1] * tp for w in weights))
        pair = pair.reshape(fs, -1, pair.shape[-1])
        ob = ob.reshape(fs, -1, ob.shape[-1])
        f32 = jnp.float32
        shapes = (
            *(jax.ShapeDtypeStruct(w.shape, f32) for w in weights),
            *(jax.ShapeDtypeStruct(w.shape, w.dtype) for w in wholes),
            *(jax.ShapeDtypeStruct(m.shape, f32) for m in means),
            *(jax.ShapeDtypeStruct(m.shape, f32) for m in olds),
        )
        vmem = pl.BlockSpec(memory_space=pltpu.VMEM)
        return pl.pallas_call(
            functools.partial(last_kernel, entries),
            out_shape=shapes,
            in_specs=[vmem] * 13,
            out_specs=(pl.BlockSpec(memory_space=pl.ANY),) * 12,
            scratch_shapes=[
                *(pltpu.VMEM(s.shape, s.dtype) for s in shapes),
                pltpu.SemaphoreType.DMA((9 + 3 * fs,)),
            ],
            compiler_params=pltpu.CompilerParams(vmem_limit_bytes=VMEM_LAST),
        )(*wholes, pair, ob, proj, squares, *means, *olds)

    return local


def solution(mesh):
    rows, split_both, columns = P("fs", None), P("fs", "tp"), P(None, "tp")
    in_specs = (rows,) * 2 + (split_both,) * 6 + (rows,) * 3 + (columns,) * 6
    out_specs = (split_both,) * 3 + (columns,) * 9
    return jax.shard_map(
        body(mesh.shape["fs"], mesh.shape["tp"]),
        mesh=mesh,
        in_specs=in_specs,
        out_specs=out_specs,
        check_vma=False,
    )
```

```python
import functools

import jax
import jax.numpy as jnp
from jax import lax
from jax.experimental import pallas as pl
from jax.experimental.pallas import tpu as pltpu
from jax.sharding import PartitionSpec as P

beta_first = 0.8
beta_second = 0.9
floor_mean = 0.005
learn_rate = 0.05

MESH = pl.DeviceIdType.MESH
LINE_CHUNKS = 5
CHUNKS = 4


def matmul(left, right):
    return jnp.dot(left, right, preferred_element_type=jnp.float32)


def moments(projected, mean_old, square_old):
    moment_one = beta_first * mean_old + (1.0 - beta_first) * projected
    moment_two = beta_second * square_old + (1.0 - beta_second) * projected * projected
    return (moment_one, moment_two, moment_one / jnp.sqrt(moment_two))


def aligned(start, size):
    return pl.ds(pl.multiple_of(start, size), size)


class Weights:
    def __init__(self, wholes, fs, me, send_sem, recv_sem):
        self.wholes, self.fs, self.me = wholes, fs, me
        self.send_sem, self.recv_sem = send_sem, recv_sem
        self.relayed = fs == 8
        self.place, self.side = me // 2, lax.rem(me, 2)

    def index(self, step, other=False):
        place = lax.rem(self.place + step + 4, 4)
        return place * 2 + (1 - self.side if other else self.side)

    def slot(self, w, i, origin):
        whole = self.wholes[w]
        block = whole.shape[0] // self.fs
        rows = block // CHUNKS
        return whole.at[aligned(origin * block + i * rows, rows), :]

    def copy(self, w, i, origin, site, role, target):
        return pltpu.make_async_remote_copy(
            src_ref=self.slot(w, i, origin),
            dst_ref=self.slot(w, i, origin),
            send_sem=self.send_sem.at[w, i, site],
            recv_sem=self.recv_sem.at[w, i, role],
            device_id={"fs": target},
            device_id_type=MESH,
        )

    def arrive(self, w, i, origin, role, inside):
        copy = self.copy(w, i, origin, 0, role, lax.rem(self.me + 1, self.fs))
        if inside is True:
            copy.wait_recv()
        else:
            pl.when(inside)(copy.wait_recv)

    def sites(self, w, i):
        p = self.place
        line = i * len(self.wholes) + w < LINE_CHUNKS
        out = [
            (0, self.me, 0, self.index(1), p < 3),
            (1, self.me, 3, self.index(-1), p > 0),
            (2, self.me, 6, self.index(0, True), True),
        ]
        cross = self.index(0, True)
        for d in (1, 2):
            out.append((2 + d, self.index(-d), d, self.index(1), (p >= d) & (p < 3)))
            out.append((4 + d, self.index(d), 3 + d, self.index(-1), (p + d < 4) & (p > 0)))
        for d in (1, 2, 3):
            below, above = p >= d, p + d < 4
            if d == 1:
                below = below & jnp.logical_not(line | (p == 1))
                above = above & jnp.logical_not(line | (p == 2))
            out.append((6 + d, self.index(-d), 6 + d, cross, below))
            out.append((9 + d, self.index(d), 9 + d, cross, above))
        out.append((13, cross, 7, self.index(1), (p < 3) & (line | (p == 0))))
        out.append((14, cross, 10, self.index(-1), (p > 0) & (line | (p == 3))))
        return {site[0]: site for site in out}

    def direct(self, w, i):
        return {
            k - 1: (k - 1, self.me, k - 1, lax.rem(self.me + k, self.fs), True)
            for k in range(1, self.fs)
        }

    def send(self, w, i, *wanted):
        table = self.sites(w, i)
        for site in wanted:
            number, origin, role, target, inside = table[site]
            copy = self.copy(w, i, origin, number, role, target)
            if inside is True:
                copy.start()
            else:
                pl.when(inside)(copy.start)

    def each(self, step):
        def chunk(i, carry):
            for w in range(len(self.wholes)):
                step(w, i)
            return carry

        lax.fori_loop(0, CHUNKS, chunk, 0)

    def start(self):
        def step(w, i):
            if self.relayed:
                self.send(w, i, 0, 1, 2)
            else:
                for number, origin, role, target, _ in self.direct(w, i).values():
                    self.copy(w, i, origin, number, role, target).start()

        self.each(step)

    def relay(self, d):
        if not self.relayed:
            return
        p = self.place

        def step(w, i):
            self.arrive(w, i, self.index(-d), d - 1, p >= d)
            self.send(w, i, *((2 + d, 6 + d) if d < 3 else (6 + d,)))
            self.arrive(w, i, self.index(d), 2 + d, p + d < 4)
            self.send(w, i, *((4 + d, 9 + d) if d < 3 else (9 + d,)))

        self.each(step)

    def relay_cross(self):
        if not self.relayed:
            return

        def step(w, i):
            self.arrive(w, i, self.index(0, True), 6, True)
            self.send(w, i, 13, 14)

        self.each(step)

    def finish(self):
        p = self.place

        def step(w, i):
            if not self.relayed:
                for k in range(1, self.fs):
                    self.arrive(w, i, lax.rem(self.me + self.fs - k, self.fs), k - 1, True)
                for number, origin, role, target, _ in self.direct(w, i).values():
                    self.copy(w, i, origin, number, role, target).wait_send()
                return
            for d in (1, 2, 3):
                self.arrive(w, i, self.index(-d, True), 6 + d, p >= d)
                self.arrive(w, i, self.index(d, True), 9 + d, p + d < 4)
            for number, origin, role, target, inside in self.sites(w, i).values():
                copy = self.copy(w, i, origin, number, role, target)
                if inside is True:
                    copy.wait_send()
                else:
                    pl.when(inside)(copy.wait_send)

        self.each(step)


def remote(ref_from, ref_to, send, recv, **device):
    return pltpu.make_async_remote_copy(
        src_ref=ref_from,
        dst_ref=ref_to,
        send_sem=send,
        recv_sem=recv,
        device_id=device,
        device_id_type=MESH,
    )


def kernel(
    fs,
    tp,
    owners,
    mixer_hbm,
    cell_hbm,
    qg_hbm,
    vg_hbm,
    og_hbm,
    qb_hbm,
    vb_hbm,
    ob_hbm,
    qw_hbm,
    vw_hbm,
    ow_hbm,
    qm_hbm,
    vm_hbm,
    om_hbm,
    qs_hbm,
    vs_hbm,
    os_hbm,
    qw_all,
    vw_all,
    ow_all,
    pair_all,
    ob_all,
    firsts,
    seconds,
    dirs,
    squares,
    mixer,
    cell,
    qg,
    vg,
    og,
    qw,
    vw,
    ow,
    means,
    olds,
    proj,
    part,
    parts,
    square_own,
    square_in,
    w_send,
    w_recv,
    b_send,
    b_recv,
    y_send,
    y_recv,
    c_send,
    c_recv,
    sum_send,
    sum_recv,
    back_send,
    back_recv,
    tp_send,
    tp_recv,
    local_sem,
):
    me, column = lax.axis_index("fs"), lax.axis_index("tp")
    rank, width = qm_hbm.shape
    far, core = column // 2, lax.rem(column, 2)
    fars = tp // 2
    own_bases = (pair_all.at[me, far, core], ob_all.at[me, far, core])
    pair_rows, ob_rows = pair_all.shape[3], ob_all.shape[3]
    pair_from = aligned(column * pair_rows, pair_rows)
    ob_from = aligned(column * ob_rows, ob_rows)
    loads = [
        pltpu.make_async_copy(source, target, local_sem.at[i])
        for i, (source, target) in enumerate(
            (
                (qb_hbm.at[pair_from, :], pair_all.at[me, far, core, :, pl.ds(0, rank)]),
                (vb_hbm.at[pair_from, :], pair_all.at[me, far, core, :, pl.ds(rank, rank)]),
                (ob_hbm.at[ob_from, :], own_bases[1]),
                (qw_hbm, qw),
                (vw_hbm, vw),
                (ow_hbm, ow),
                (mixer_hbm, mixer),
                (cell_hbm, cell),
                (qg_hbm, qg),
                (vg_hbm, vg),
                (og_hbm, og),
                (qm_hbm, means.at[:, pl.ds(0, width)]),
                (vm_hbm, means.at[:, pl.ds(width, width)]),
                (om_hbm, means.at[:, pl.ds(2 * width, 2 * width)]),
                (qs_hbm, olds.at[:, pl.ds(0, width)]),
                (vs_hbm, olds.at[:, pl.ds(width, width)]),
                (os_hbm, olds.at[:, pl.ds(2 * width, 2 * width)]),
            )
        )
    ]
    for load in loads:
        load.start()

    barrier = pltpu.get_barrier_semaphore()
    for k in range(1, fs):
        pl.semaphore_signal(
            barrier, inc=1, device_id={"fs": lax.rem(me + k, fs)}, device_id_type=MESH
        )
    for k in range(1, tp):
        pl.semaphore_signal(
            barrier, inc=1, device_id={"tp": lax.rem(column + k, tp)}, device_id_type=MESH
        )
    pl.semaphore_wait(barrier, fs + tp - 2)

    for load in loads[:3]:
        load.wait()
    bases = (pair_all, ob_all)
    sent = []
    for k in range(1, fs):
        for n, whole in enumerate(bases):
            mine = whole.at[me, far, core]
            copy = remote(
                mine,
                mine,
                b_send.at[n, k - 1],
                b_recv.at[n, k - 1],
                fs=lax.rem(me + k, fs),
            )
            copy.start()
            sent.append(copy)

    for load in loads[3:6]:
        load.wait()
    wholes = (qw_all, vw_all, ow_all)
    for own, whole in zip((qw, vw, ow), wholes):
        block = own.shape[0]
        whole[aligned(me * block, block), :] = own[...].astype(jnp.bfloat16)
    weights = Weights(wholes, fs, me, w_send, w_recv)
    weights.start()
    part[...] = jnp.zeros_like(part)

    for k in range(1, fs):
        source = lax.rem(me + fs - k, fs)
        for n, whole in enumerate(bases):
            there = whole.at[source, far, core]
            remote(
                there,
                there,
                b_send.at[n, k - 1],
                b_recv.at[n, k - 1],
                fs=lax.rem(me + k, fs),
            ).wait_recv()
    for k in range(1, fars):
        for n, whole in enumerate(bases):
            mine = whole.at[:, far, core]
            copy = remote(
                mine,
                mine,
                y_send.at[n, k - 1],
                y_recv.at[n, k - 1],
                tp=lax.rem(far + k, fars) * 2 + core,
            )
            copy.start()
            sent.append(copy)
    for k in range(1, fars):
        source = lax.rem(far + fars - k, fars)
        for n, whole in enumerate(bases):
            there = whole.at[:, source, core]
            remote(
                there,
                there,
                y_send.at[n, k - 1],
                y_recv.at[n, k - 1],
                tp=lax.rem(far + k, fars) * 2 + core,
            ).wait_recv()
    for n, whole in enumerate(bases):
        mine = whole.at[:, :, core]
        copy = remote(mine, mine, c_send.at[n], c_recv.at[n], tp=far * 2 + 1 - core)
        copy.start()
        sent.append(copy)
    for load in loads[6:]:
        load.wait()
    for n, whole in enumerate(bases):
        there = whole.at[:, :, 1 - core]
        remote(there, there, c_send.at[n], c_recv.at[n], tp=far * 2 + 1 - core).wait_recv()

    tile = 256

    def project(rows, grad):
        turned = jnp.transpose(rows)
        high = turned.astype(jnp.bfloat16)
        low = (turned - high.astype(jnp.float32)).astype(jnp.bfloat16)
        both = matmul(jnp.concatenate([high, low], axis=0), grad)
        return both[:rank] + both[rank:]

    def flat(ref):
        value = ref[...]
        return value.reshape(-1, value.shape[-1])

    def step(t, carry):
        at = aligned(t * tile, tile)
        rows = matmul(mixer[at, :], flat(pair_all))
        part[:, :width] += project(rows[:, :rank], qg[at, :])
        part[:, width : 2 * width] += project(rows[:, rank:], vg[at, :])
        part[:, 2 * width :] += project(matmul(cell[at, :], flat(ob_all)), og[at, :])
        return carry

    lax.fori_loop(0, mixer.shape[0] // tile, step, 0)

    first_owner = (fs - owners) // 2
    share = rank // owners

    def owns(index):
        return (index >= first_owner) & (index < first_owner + owners)

    def strip_of(index):
        return lax.rem(index - first_owner + fs, owners)

    def strip(index):
        return aligned(strip_of(index) * share, share)

    drains = []
    for k in range(1, fs):
        target = lax.rem(me + k, fs)
        copy = remote(
            part.at[strip(target), :],
            parts.at[k - 1],
            sum_send.at[k - 1],
            sum_recv.at[k - 1],
            fs=target,
        )
        pl.when(owns(target))(copy.start)
        drains.append((copy, owns(target)))

    weights.relay(1)

    def gram(ref):
        rows, size = ref.shape[3], ref.shape[4]

        def add(i, total):
            piece = ref[i].reshape(-1, size)
            turned = jnp.transpose(piece.astype(jnp.float32)).astype(jnp.bfloat16)
            return total + matmul(turned, piece)

        return lax.fori_loop(0, ref.shape[0], add, jnp.zeros((size, size), jnp.float32))

    gram_pair = gram(pair_all)
    gram_output = gram(ob_all)

    back = []
    for k in range(1, fs):
        target = lax.rem(me + k, fs)
        mine = proj.at[strip(me), :]
        back.append(
            remote(mine, mine, back_send.at[k - 1], back_recv.at[k - 1], fs=target)
        )

    @pl.when(owns(me))
    def _():
        for k in range(1, fs):
            remote(
                part.at[strip(me), :],
                parts.at[k - 1],
                sum_send.at[k - 1],
                sum_recv.at[k - 1],
                fs=lax.rem(me + k, fs),
            ).wait_recv()
        total = part[strip(me), :]
        for k in range(1, fs):
            total = total + parts[k - 1]
        proj[strip(me), :] = total.astype(proj.dtype)
        for copy in back:
            copy.start()

    weights.relay(2)
    weights.relay_cross()
    weights.relay(3)

    for k in range(1, fs):
        source = lax.rem(me + fs - k, fs)
        there = proj.at[strip(source), :]
        copy = remote(
            there, there, back_send.at[k - 1], back_recv.at[k - 1], fs=lax.rem(me + k, fs)
        )
        pl.when(owns(source))(copy.wait_recv)

    def norm(basis_gram, left, columns):
        at = pl.ds(left, columns)
        first, second, direction = moments(
            proj[:, at].astype(jnp.float32), means[:, at], olds[:, at]
        )
        firsts[:, at] = first
        seconds[:, at] = second
        high = direction.astype(jnp.bfloat16)
        dirs[:rank, at] = high
        dirs[rank:, at] = (direction - high.astype(jnp.float32)).astype(jnp.bfloat16)
        turned = jnp.dot(
            basis_gram,
            direction,
            precision=lax.Precision.HIGHEST,
            preferred_element_type=jnp.float32,
        )
        lanes = jnp.sum(direction * turned, axis=0, keepdims=True)
        return jnp.sum(lanes, axis=1, keepdims=True)

    partial = (
        norm(gram_pair[:rank, :rank], 0, width)
        + norm(gram_pair[rank:, rank:], width, width)
        + norm(gram_output, 2 * width, 2 * width)
    )
    square_own[...] = jnp.broadcast_to(partial, square_own.shape)
    shares = []
    for k in range(1, tp):
        copy = remote(
            square_own,
            square_in.at[k - 1],
            tp_send.at[k - 1],
            tp_recv.at[k - 1],
            tp=lax.rem(column + k, tp),
        )
        copy.start()
        shares.append(copy)

    for copy in shares:
        copy.wait_recv()
    whole_squares = square_own[...]
    for k in range(1, tp):
        whole_squares = whole_squares + square_in[k - 1]
    squares[...] = whole_squares
    weights.finish()
    for copy in sent + shares:
        copy.wait_send()
    for copy, inside in drains:
        pl.when(inside)(copy.wait_send)

    @pl.when(owns(me))
    def _():
        for copy in back:
            copy.wait_send()


def exchange(fs, tp, mixer, cell, grads, bases, weights, means, olds):
    rank = means[0].shape[0]
    total = sum(grad.shape[1] for grad in grads)
    owners = min(4, fs)
    bf16, f32 = jnp.bfloat16, jnp.float32
    hbm, vmem = pl.BlockSpec(memory_space=pltpu.HBM), pl.BlockSpec(memory_space=pltpu.VMEM)
    dma = pltpu.SemaphoreType.DMA

    def whole(array):
        return jax.ShapeDtypeStruct((array.shape[0] * fs, array.shape[1]), bf16)

    def parted(array, columns):
        return jax.ShapeDtypeStruct((fs, tp // 2, 2, array.shape[0] // tp, columns), bf16)

    return pl.pallas_call(
        functools.partial(kernel, fs, tp, owners),
        out_shape=(
            *(whole(weight) for weight in weights),
            parted(bases[0], 2 * rank),
            parted(bases[2], rank),
            jax.ShapeDtypeStruct((rank, total), f32),
            jax.ShapeDtypeStruct((rank, total), f32),
            jax.ShapeDtypeStruct((2 * rank, total), bf16),
            jax.ShapeDtypeStruct((8, 128), f32),
        ),
        in_specs=[hbm] * 17,
        out_specs=(vmem,) * 9,
        scratch_shapes=[
            *(pltpu.VMEM(array.shape, bf16) for array in (mixer, cell, *grads)),
            *(pltpu.VMEM(array.shape, f32) for array in weights),
            pltpu.VMEM((rank, total), f32),
            pltpu.VMEM((rank, total), f32),
            pltpu.VMEM((rank, total), bf16),
            pltpu.VMEM((rank, total), f32),
            pltpu.VMEM((fs - 1, rank // owners, total), f32),
            pltpu.VMEM((8, 128), f32),
            pltpu.VMEM((tp - 1, 8, 128), f32),
            dma((3, CHUNKS, max(15, fs - 1))),
            dma((3, CHUNKS, max(13, fs - 1))),
            dma((2, fs - 1)),
            dma((2, fs - 1)),
            dma((2, max(1, tp // 2 - 1))),
            dma((2, max(1, tp // 2 - 1))),
            dma((2,)),
            dma((2,)),
            dma((fs - 1,)),
            dma((fs - 1,)),
            dma((fs - 1,)),
            dma((fs - 1,)),
            dma((tp - 1,)),
            dma((tp - 1,)),
            dma((17,)),
        ],
        compiler_params=pltpu.CompilerParams(
            collective_id=0, has_side_effects=True, vmem_limit_bytes=VMEM_MAIN
        ),
    )(*(pltpu.with_memory_space_constraint(a, pltpu.HBM) for a in (mixer, cell, *grads, *bases, *weights, *means, *olds)))


VMEM_MAIN = 30 * 1024 * 1024
VMEM_LAST = 24 * 1024 * 1024


def last_kernel(entries, *refs):
    wholes, (pair, ob, firsts, seconds, dirs, squares) = refs[:3], refs[3:9]
    outputs, stage, sem = refs[9:21], refs[21:27], refs[27]
    rank = pair.shape[2] // 2
    me = lax.axis_index("fs")
    copies = []

    def put(source, target):
        copy = pltpu.make_async_copy(source, target, sem.at[len(copies)])
        copy.start()
        copies.append(copy)

    cuts, left = [], 0
    for whole in wholes:
        cuts.append(pl.ds(left, whole.shape[1]))
        left += whole.shape[1]
    for n, cut in enumerate(cuts):
        put(firsts.at[:, cut], outputs[6 + n])
        put(seconds.at[:, cut], outputs[9 + n])
    factor = 1.0 / jnp.sqrt(squares[0:1, 0:1] / entries + floor_mean)
    scale = -learn_rate * factor
    bases = ((pair, 0), (pair, rank), (ob, 0))
    for n, (cut, (base, low)) in enumerate(zip(cuts, bases)):
        both = dirs[:, cut]
        own = base[me, :, low : low + rank]
        stage[n][...] = -factor * matmul(jnp.concatenate([own, own], axis=1), both)
        put(stage[n], outputs[n])
        high = both[:rank]
        block = base.shape[1]
        for o in range(base.shape[0]):
            rows = pl.ds(o * block, block)
            update = matmul(base[o, :, low : low + rank], high)
            stage[3 + n][rows, :] = (
                wholes[n][rows, :].astype(jnp.float32) + scale * update
            ).astype(jnp.bfloat16)
            put(stage[3 + n].at[rows, :], outputs[3 + n].at[rows, :])
    for copy in copies:
        copy.wait()


def body(fs, tp):
    def local(
        mixer_input,
        cell_output,
        query_grad,
        value_grad,
        output_grad,
        query_weight,
        value_weight,
        output_weight,
        query_basis,
        value_basis,
        output_basis,
        query_mean,
        value_mean,
        output_mean,
        query_square,
        value_square,
        output_square,
    ):
        means = (query_mean, value_mean, output_mean)
        olds = (query_square, value_square, output_square)
        weights = (query_weight, value_weight, output_weight)
        *wholes, pair, ob, firsts, seconds, dirs, squares = exchange(
            fs,
            tp,
            mixer_input,
            cell_output,
            (query_grad, value_grad, output_grad),
            (query_basis, value_basis, output_basis),
            weights,
            means,
            olds,
        )
        entries = float(sum(w.shape[0] * fs * w.shape[1] * tp for w in weights))
        pair = pair.reshape(fs, -1, pair.shape[-1])
        ob = ob.reshape(fs, -1, ob.shape[-1])
        f32 = jnp.float32
        shapes = (
            *(jax.ShapeDtypeStruct(w.shape, f32) for w in weights),
            *(jax.ShapeDtypeStruct(w.shape, w.dtype) for w in wholes),
            *(jax.ShapeDtypeStruct(m.shape, f32) for m in means),
            *(jax.ShapeDtypeStruct(m.shape, f32) for m in olds),
        )
        vmem = pl.BlockSpec(memory_space=pltpu.VMEM)
        return pl.pallas_call(
            functools.partial(last_kernel, entries),
            out_shape=shapes,
            in_specs=[vmem] * 9,
            out_specs=(pl.BlockSpec(memory_space=pl.ANY),) * 12,
            scratch_shapes=[
                *(pltpu.VMEM(s.shape, s.dtype) for s in shapes[:6]),
                pltpu.SemaphoreType.DMA((9 + 3 * fs,)),
            ],
            compiler_params=pltpu.CompilerParams(vmem_limit_bytes=VMEM_LAST),
        )(*wholes, pair, ob, firsts, seconds, dirs, squares)

    return local


def solution(mesh):
    rows, split_both, columns = P("fs", None), P("fs", "tp"), P(None, "tp")
    in_specs = (rows,) * 2 + (split_both,) * 6 + (rows,) * 3 + (columns,) * 6
    out_specs = (split_both,) * 3 + (columns,) * 9
    return jax.shard_map(
        body(mesh.shape["fs"], mesh.shape["tp"]),
        mesh=mesh,
        in_specs=in_specs,
        out_specs=out_specs,
        check_vma=False,
    )
```

```python
import functools

import jax
import jax.numpy as jnp
from jax import lax
from jax.experimental import pallas as pl
from jax.experimental.pallas import tpu as pltpu
from jax.sharding import PartitionSpec as P

beta_first = 0.8
beta_second = 0.9
floor_mean = 0.005
learn_rate = 0.05

MESH = pl.DeviceIdType.MESH
LINE_CHUNKS = 7
BASE_LINE = (False, True)
CHUNKS = 4


def matmul(left, right):
    return jnp.dot(left, right, preferred_element_type=jnp.float32)


def moments(projected, mean_old, square_old):
    moment_one = beta_first * mean_old + (1.0 - beta_first) * projected
    moment_two = beta_second * square_old + (1.0 - beta_second) * projected * projected
    return (moment_one, moment_two, moment_one / jnp.sqrt(moment_two))


def aligned(start, size):
    return pl.ds(pl.multiple_of(start, size), size)


class Gather:
    def __init__(self, fs, me, count, chunks, slot, line, send_sem, recv_sem):
        self.fs, self.me, self.count, self.chunks = fs, me, count, chunks
        self.slot, self.line = slot, line
        self.send_sem, self.recv_sem = send_sem, recv_sem
        self.relayed = fs == 8
        self.place, self.side = me // 2, lax.rem(me, 2)

    def index(self, step, other=False):
        place = lax.rem(self.place + step + 4, 4)
        return place * 2 + (1 - self.side if other else self.side)

    def copy(self, w, i, origin, site, role, target):
        return pltpu.make_async_remote_copy(
            src_ref=self.slot(w, i, origin),
            dst_ref=self.slot(w, i, origin),
            send_sem=self.send_sem.at[w, i, site],
            recv_sem=self.recv_sem.at[w, i, role],
            device_id={"fs": target},
            device_id_type=MESH,
        )

    def arrive(self, w, i, origin, role, inside=True):
        copy = self.copy(w, i, origin, 0, role, lax.rem(self.me + 1, self.fs))
        if inside is True:
            copy.wait_recv()
        else:
            pl.when(inside)(copy.wait_recv)

    def sites(self, w, i):
        p = self.place
        line = self.line(w, i)
        out = [
            (0, self.me, 0, self.index(1), p < 3),
            (1, self.me, 3, self.index(-1), p > 0),
            (2, self.me, 6, self.index(0, True), True),
        ]
        cross = self.index(0, True)
        for d in (1, 2):
            out.append((2 + d, self.index(-d), d, self.index(1), (p >= d) & (p < 3)))
            out.append((4 + d, self.index(d), 3 + d, self.index(-1), (p + d < 4) & (p > 0)))
        for d in (1, 2, 3):
            below, above = p >= d, p + d < 4
            if d == 1:
                below = below & jnp.logical_not(line | (p == 1))
                above = above & jnp.logical_not(line | (p == 2))
            out.append((6 + d, self.index(-d), 6 + d, cross, below))
            out.append((9 + d, self.index(d), 9 + d, cross, above))
        out.append((13, cross, 7, self.index(1), (p < 3) & (line | (p == 0))))
        out.append((14, cross, 10, self.index(-1), (p > 0) & (line | (p == 3))))
        return {site[0]: site for site in out}

    def direct(self):
        return [(k - 1, lax.rem(self.me + k, self.fs)) for k in range(1, self.fs)]

    def send(self, w, i, wanted, also=None):
        table = self.sites(w, i)
        for site in wanted:
            number, origin, role, target, inside = table[site]
            copy = self.copy(w, i, origin, number, role, target)
            if also is not None:
                inside = inside & also
            if inside is True:
                copy.start()
            else:
                pl.when(inside)(copy.start)

    def each(self, step, low=0, high=None, only=None):
        high = self.chunks if high is None else high

        def chunk(i, carry):
            for w in range(self.count) if only is None else (only,):
                step(w, i)
            return carry

        if high - low == 1:
            chunk(low, 0)
        elif high > low:
            lax.fori_loop(low, high, chunk, 0)

    def start(self, low=0, high=None, only=None):
        def step(w, i):
            if self.relayed:
                self.send(w, i, (0, 1, 2))
            else:
                for number, target in self.direct():
                    self.copy(w, i, self.me, number, number, target).start()

        self.each(step, low, high, only)

    def relay_out(self, low=0, high=None):
        p = self.place

        def step(w, i):
            self.arrive(w, i, self.index(-1), 0, p >= 2)
            self.send(w, i, (3, 7), p >= 2)
            self.arrive(w, i, self.index(1), 3, p <= 1)
            self.send(w, i, (5, 10), p <= 1)

        if self.relayed:
            self.each(step, low, high)

    def relay_in(self, low=0, high=None):
        p = self.place

        def step(w, i):
            self.arrive(w, i, self.index(-1), 0, p == 1)
            self.send(w, i, (3,), p == 1)
            self.arrive(w, i, self.index(1), 3, p == 2)
            self.send(w, i, (5,), p == 2)

        if self.relayed:
            self.each(step, low, high)

    def relay(self, d, low=0, high=None):
        p = self.place

        def step(w, i):
            self.arrive(w, i, self.index(-d), d - 1, p >= d)
            self.send(w, i, (2 + d, 6 + d) if d < 3 else (6 + d,))
            self.arrive(w, i, self.index(d), 2 + d, p + d < 4)
            self.send(w, i, (4 + d, 9 + d) if d < 3 else (9 + d,))

        if self.relayed:
            self.each(step, low, high)

    def relay_cross(self):
        def step(w, i):
            self.arrive(w, i, self.index(0, True), 6)
            self.send(w, i, (13, 14))

        if self.relayed:
            self.each(step)

    def finish(self):
        p = self.place

        def step(w, i):
            if not self.relayed:
                for k in range(1, self.fs):
                    self.arrive(w, i, lax.rem(self.me + self.fs - k, self.fs), k - 1)
                return
            for d in (1, 2, 3):
                self.arrive(w, i, self.index(-d, True), 6 + d, p >= d)
                self.arrive(w, i, self.index(d, True), 9 + d, p + d < 4)

        self.each(step)

    def drain(self):
        def step(w, i):
            if not self.relayed:
                for number, target in self.direct():
                    self.copy(w, i, self.me, number, number, target).wait_send()
                return
            for number, origin, role, target, inside in self.sites(w, i).values():
                copy = self.copy(w, i, origin, number, role, target)
                if inside is True:
                    copy.wait_send()
                else:
                    pl.when(inside)(copy.wait_send)

        self.each(step)


def remote(ref_from, ref_to, send, recv, **device):
    return pltpu.make_async_remote_copy(
        src_ref=ref_from,
        dst_ref=ref_to,
        send_sem=send,
        recv_sem=recv,
        device_id=device,
        device_id_type=MESH,
    )


def kernel(
    fs,
    tp,
    owners,
    mixer_hbm,
    cell_hbm,
    qg_hbm,
    vg_hbm,
    og_hbm,
    qb_hbm,
    vb_hbm,
    ob_hbm,
    qw_hbm,
    vw_hbm,
    ow_hbm,
    qm_hbm,
    vm_hbm,
    om_hbm,
    qs_hbm,
    vs_hbm,
    os_hbm,
    qw_all,
    vw_all,
    ow_all,
    pair_all,
    ob_all,
    firsts,
    seconds,
    dirs,
    squares,
    mixer,
    cell,
    qg,
    vg,
    og,
    qw,
    vw,
    ow,
    means,
    olds,
    proj,
    part,
    parts,
    square_own,
    square_in,
    w_send,
    w_recv,
    b_send,
    b_recv,
    y_send,
    y_recv,
    c_send,
    c_recv,
    sum_send,
    sum_recv,
    back_send,
    back_recv,
    over_send,
    tp_send,
    tp_recv,
    local_sem,
):
    me, column = lax.axis_index("fs"), lax.axis_index("tp")
    rank, width = qm_hbm.shape
    far, core = column // 2, lax.rem(column, 2)
    fars = tp // 2
    own_bases = (pair_all.at[me, far, core], ob_all.at[me, far, core])
    pair_rows, ob_rows = pair_all.shape[3], ob_all.shape[3]
    pair_from = aligned(column * pair_rows, pair_rows)
    ob_from = aligned(column * ob_rows, ob_rows)
    loads = [
        pltpu.make_async_copy(source, target, local_sem.at[i])
        for i, (source, target) in enumerate(
            (
                (qb_hbm.at[pair_from, :], pair_all.at[me, far, core, :, pl.ds(0, rank)]),
                (vb_hbm.at[pair_from, :], pair_all.at[me, far, core, :, pl.ds(rank, rank)]),
                (ob_hbm.at[ob_from, :], own_bases[1]),
                (qw_hbm, qw),
                (vw_hbm, vw),
                (ow_hbm, ow),
                (mixer_hbm, mixer),
                (cell_hbm, cell),
                (qg_hbm, qg),
                (vg_hbm, vg),
                (og_hbm, og),
                (qm_hbm, means.at[:, pl.ds(0, width)]),
                (vm_hbm, means.at[:, pl.ds(width, width)]),
                (om_hbm, means.at[:, pl.ds(2 * width, 2 * width)]),
                (qs_hbm, olds.at[:, pl.ds(0, width)]),
                (vs_hbm, olds.at[:, pl.ds(width, width)]),
                (os_hbm, olds.at[:, pl.ds(2 * width, 2 * width)]),
            )
        )
    ]
    for load in loads:
        load.start()

    barrier = pltpu.get_barrier_semaphore()
    for k in range(1, fs):
        pl.semaphore_signal(
            barrier, inc=1, device_id={"fs": lax.rem(me + k, fs)}, device_id_type=MESH
        )
    for k in range(1, tp):
        pl.semaphore_signal(
            barrier, inc=1, device_id={"tp": lax.rem(column + k, tp)}, device_id_type=MESH
        )
    pl.semaphore_wait(barrier, fs + tp - 2)

    for load in loads[:3]:
        load.wait()
    bases = (pair_all, ob_all)
    wholes = (qw_all, vw_all, ow_all)
    sent = []

    def base_slot(w, i, origin):
        return bases[w].at[origin, far, core]

    def weight_slot(w, i, origin):
        block = wholes[w].shape[0] // fs
        rows = block // CHUNKS
        return wholes[w].at[aligned(origin * block + i * rows, rows), :]

    parts_of_bases = Gather(
        fs, me, 2, 1, base_slot, lambda w, i: BASE_LINE[w], b_send, b_recv
    )
    weights = Gather(
        fs,
        me,
        3,
        CHUNKS,
        weight_slot,
        lambda w, i: i * len(wholes) + w < LINE_CHUNKS,
        w_send,
        w_recv,
    )
    parts_of_bases.start()
    for load in loads[3:6]:
        load.wait()
    for own, whole in zip((qw, vw, ow), wholes):
        block = own.shape[0]
        whole[aligned(me * block, block), :] = own[...].astype(jnp.bfloat16)
    weights.start(0, 1, 0)
    part[...] = jnp.zeros_like(part)
    parts_of_bases.relay(1)
    parts_of_bases.relay_cross()
    weights.start(0, 1, 1)
    parts_of_bases.relay(2)
    weights.start(0, 1, 2)
    parts_of_bases.relay(3)
    weights.start(1)
    parts_of_bases.finish()
    for k in range(1, fars):
        for n, whole in enumerate(bases):
            mine = whole.at[:, far, core]
            copy = remote(
                mine,
                mine,
                y_send.at[n, k - 1],
                y_recv.at[n, k - 1],
                tp=lax.rem(far + k, fars) * 2 + core,
            )
            copy.start()
            sent.append(copy)
    weights.relay_out(0, 2)
    for k in range(1, fars):
        source = lax.rem(far + fars - k, fars)
        for n, whole in enumerate(bases):
            there = whole.at[:, source, core]
            remote(
                there,
                there,
                y_send.at[n, k - 1],
                y_recv.at[n, k - 1],
                tp=lax.rem(far + k, fars) * 2 + core,
            ).wait_recv()
    for n, whole in enumerate(bases):
        mine = whole.at[:, :, core]
        copy = remote(mine, mine, c_send.at[n], c_recv.at[n], tp=far * 2 + 1 - core)
        copy.start()
        sent.append(copy)
    for load in loads[6:]:
        load.wait()
    for n, whole in enumerate(bases):
        there = whole.at[:, :, 1 - core]
        remote(there, there, c_send.at[n], c_recv.at[n], tp=far * 2 + 1 - core).wait_recv()

    tile = 256

    def project(rows, grad):
        turned = jnp.transpose(rows)
        high = turned.astype(jnp.bfloat16)
        low = (turned - high.astype(jnp.float32)).astype(jnp.bfloat16)
        both = matmul(jnp.concatenate([high, low], axis=0), grad)
        return both[:rank] + both[rank:]

    def flat(ref):
        value = ref[...]
        return value.reshape(-1, value.shape[-1])

    def step(t, carry):
        at = aligned(t * tile, tile)
        rows = matmul(mixer[at, :], flat(pair_all))
        part[:, :width] += project(rows[:, :rank], qg[at, :])
        part[:, width : 2 * width] += project(rows[:, rank:], vg[at, :])
        part[:, 2 * width :] += project(matmul(cell[at, :], flat(ob_all)), og[at, :])
        return carry

    lax.fori_loop(0, mixer.shape[0] // tile, step, 0)

    first_owner = (fs - owners) // 2
    share = rank // owners

    def owns(index):
        return (index >= first_owner) & (index < first_owner + owners)

    def strip_of(index):
        return lax.rem(index - first_owner + fs, owners)

    def strip(index):
        return aligned(strip_of(index) * share, share)

    drains = []
    for k in range(1, fs):
        target = lax.rem(me + k, fs)
        copy = remote(
            part.at[strip(target), :],
            parts.at[k - 1],
            sum_send.at[k - 1],
            sum_recv.at[k - 1],
            fs=target,
        )
        pl.when(owns(target))(copy.start)
        drains.append((copy, owns(target)))

    weights.relay_out(2)
    weights.relay_in(0, 1)

    def gram(ref):
        rows, size = ref.shape[3], ref.shape[4]

        def add(i, total):
            piece = ref[i].reshape(-1, size)
            turned = jnp.transpose(piece.astype(jnp.float32)).astype(jnp.bfloat16)
            return total + matmul(turned, piece)

        return lax.fori_loop(0, ref.shape[0], add, jnp.zeros((size, size), jnp.float32))

    gram_pair = gram(pair_all)
    gram_output = gram(ob_all)

    side = lax.rem(me, 2)
    relayed = weights.relayed
    back = []
    for k in range(1, fs):
        target = lax.rem(me + k, fs)
        mine = proj.at[strip(me), :]
        inside = owns(me)
        if relayed:
            inside = inside & (owns(target) | (lax.rem(target, 2) == side))
        copy = remote(
            mine, mine, back_send.at[k - 1], back_recv.at[strip_of(me)], fs=target
        )
        back.append((copy, inside))
    other = me + 1 - 2 * side if relayed else lax.rem(me + 1, fs)
    returned = []
    for j in range(owners):
        there = proj.at[pl.ds(j * share, share), :]
        source = first_owner + j
        straight = me != source
        if relayed:
            same = side == source % 2
            straight = straight & (owns(me) | same)
        over = remote(there, there, over_send.at[j], back_recv.at[j], fs=other)
        returned.append((over, straight, jnp.logical_not(owns(me)) if relayed else None, source % 2))

    @pl.when(owns(me))
    def _():
        for k in range(1, fs):
            remote(
                part.at[strip(me), :],
                parts.at[k - 1],
                sum_send.at[k - 1],
                sum_recv.at[k - 1],
                fs=lax.rem(me + k, fs),
            ).wait_recv()
        total = part[strip(me), :]
        for k in range(1, fs):
            total = total + parts[k - 1]
        proj[strip(me), :] = total.astype(proj.dtype)

    for copy, inside in back:
        pl.when(inside)(copy.start)

    weights.relay_in(1)
    weights.relay(2)
    weights.relay_cross()

    for over, straight, at_end, parity in returned:
        pl.when(straight)(over.wait_recv)
        if relayed:
            pl.when(at_end & (side == parity))(over.start)
    weights.relay(3)
    if relayed:
        for over, straight, at_end, parity in returned:
            pl.when(at_end & (side != parity))(over.wait_recv)

    def norm(basis_gram, left, columns):
        at = pl.ds(left, columns)
        first, second, direction = moments(
            proj[:, at].astype(jnp.float32), means[:, at], olds[:, at]
        )
        firsts[:, at] = first
        seconds[:, at] = second
        high = direction.astype(jnp.bfloat16)
        dirs[:rank, at] = high
        dirs[rank:, at] = (direction - high.astype(jnp.float32)).astype(jnp.bfloat16)
        turned = jnp.dot(
            basis_gram,
            direction,
            precision=lax.Precision.HIGHEST,
            preferred_element_type=jnp.float32,
        )
        lanes = jnp.sum(direction * turned, axis=0, keepdims=True)
        return jnp.sum(lanes, axis=1, keepdims=True)

    partial = (
        norm(gram_pair[:rank, :rank], 0, width)
        + norm(gram_pair[rank:, rank:], width, width)
        + norm(gram_output, 2 * width, 2 * width)
    )
    square_own[...] = jnp.broadcast_to(partial, square_own.shape)
    shares = []
    for k in range(1, tp):
        copy = remote(
            square_own,
            square_in.at[k - 1],
            tp_send.at[k - 1],
            tp_recv.at[k - 1],
            tp=lax.rem(column + k, tp),
        )
        copy.start()
        shares.append(copy)

    for copy in shares:
        copy.wait_recv()
    whole_squares = square_own[...]
    for k in range(1, tp):
        whole_squares = whole_squares + square_in[k - 1]
    squares[...] = whole_squares
    weights.finish()
    for copy in sent + shares:
        copy.wait_send()
    for copy, inside in drains + back:
        pl.when(inside)(copy.wait_send)
    if relayed:
        for over, straight, at_end, parity in returned:
            pl.when(at_end & (side == parity))(over.wait_send)
    parts_of_bases.drain()
    weights.drain()


def exchange(fs, tp, mixer, cell, grads, bases, weights, means, olds):
    rank = means[0].shape[0]
    total = sum(grad.shape[1] for grad in grads)
    owners = min(4, fs)
    bf16, f32 = jnp.bfloat16, jnp.float32
    hbm, vmem = pl.BlockSpec(memory_space=pltpu.HBM), pl.BlockSpec(memory_space=pltpu.VMEM)
    dma = pltpu.SemaphoreType.DMA

    def whole(array):
        return jax.ShapeDtypeStruct((array.shape[0] * fs, array.shape[1]), bf16)

    def parted(array, columns):
        return jax.ShapeDtypeStruct((fs, tp // 2, 2, array.shape[0] // tp, columns), bf16)

    return pl.pallas_call(
        functools.partial(kernel, fs, tp, owners),
        out_shape=(
            *(whole(weight) for weight in weights),
            parted(bases[0], 2 * rank),
            parted(bases[2], rank),
            jax.ShapeDtypeStruct((rank, total), f32),
            jax.ShapeDtypeStruct((rank, total), f32),
            jax.ShapeDtypeStruct((2 * rank, total), bf16),
            jax.ShapeDtypeStruct((8, 128), f32),
        ),
        in_specs=[hbm] * 17,
        out_specs=(vmem,) * 9,
        scratch_shapes=[
            *(pltpu.VMEM(array.shape, bf16) for array in (mixer, cell, *grads)),
            *(pltpu.VMEM(array.shape, f32) for array in weights),
            pltpu.VMEM((rank, total), f32),
            pltpu.VMEM((rank, total), f32),
            pltpu.VMEM((rank, total), bf16),
            pltpu.VMEM((rank, total), f32),
            pltpu.VMEM((fs - 1, rank // owners, total), f32),
            pltpu.VMEM((8, 128), f32),
            pltpu.VMEM((tp - 1, 8, 128), f32),
            dma((3, CHUNKS, max(15, fs - 1))),
            dma((3, CHUNKS, max(13, fs - 1))),
            dma((2, 1, max(15, fs - 1))),
            dma((2, 1, max(13, fs - 1))),
            dma((2, max(1, tp // 2 - 1))),
            dma((2, max(1, tp // 2 - 1))),
            dma((2,)),
            dma((2,)),
            dma((fs - 1,)),
            dma((fs - 1,)),
            dma((fs - 1,)),
            dma((owners,)),
            dma((owners,)),
            dma((tp - 1,)),
            dma((tp - 1,)),
            dma((17,)),
        ],
        compiler_params=pltpu.CompilerParams(
            collective_id=0, has_side_effects=True, vmem_limit_bytes=VMEM_MAIN
        ),
    )(*(pltpu.with_memory_space_constraint(a, pltpu.HBM) for a in (mixer, cell, *grads, *bases, *weights, *means, *olds)))


VMEM_MAIN = 30 * 1024 * 1024
VMEM_LAST = 24 * 1024 * 1024


def last_kernel(entries, *refs):
    wholes, (pair, ob, firsts, seconds, dirs, squares) = refs[:3], refs[3:9]
    outputs, stage, sem = refs[9:21], refs[21:27], refs[27]
    rank = pair.shape[2] // 2
    me = lax.axis_index("fs")
    copies = []

    def put(source, target):
        copy = pltpu.make_async_copy(source, target, sem.at[len(copies)])
        copy.start()
        copies.append(copy)

    cuts, left = [], 0
    for whole in wholes:
        cuts.append(pl.ds(left, whole.shape[1]))
        left += whole.shape[1]
    for n, cut in enumerate(cuts):
        put(firsts.at[:, cut], outputs[6 + n])
        put(seconds.at[:, cut], outputs[9 + n])
    factor = 1.0 / jnp.sqrt(squares[0:1, 0:1] / entries + floor_mean)
    scale = -learn_rate * factor
    bases = ((pair, 0), (pair, rank), (ob, 0))
    for n, (cut, (base, low)) in enumerate(zip(cuts, bases)):
        both = dirs[:, cut]
        own = base[me, :, low : low + rank]
        stage[n][...] = -factor * matmul(jnp.concatenate([own, own], axis=1), both)
        put(stage[n], outputs[n])
        high = both[:rank]
        block = base.shape[1]
        for o in range(base.shape[0]):
            rows = pl.ds(o * block, block)
            update = matmul(base[o, :, low : low + rank], high)
            stage[3 + n][rows, :] = (
                wholes[n][rows, :].astype(jnp.float32) + scale * update
            ).astype(jnp.bfloat16)
            put(stage[3 + n].at[rows, :], outputs[3 + n].at[rows, :])
    for copy in copies:
        copy.wait()


def body(fs, tp):
    def local(
        mixer_input,
        cell_output,
        query_grad,
        value_grad,
        output_grad,
        query_weight,
        value_weight,
        output_weight,
        query_basis,
        value_basis,
        output_basis,
        query_mean,
        value_mean,
        output_mean,
        query_square,
        value_square,
        output_square,
    ):
        means = (query_mean, value_mean, output_mean)
        olds = (query_square, value_square, output_square)
        weights = (query_weight, value_weight, output_weight)
        *wholes, pair, ob, firsts, seconds, dirs, squares = exchange(
            fs,
            tp,
            mixer_input,
            cell_output,
            (query_grad, value_grad, output_grad),
            (query_basis, value_basis, output_basis),
            weights,
            means,
            olds,
        )
        entries = float(sum(w.shape[0] * fs * w.shape[1] * tp for w in weights))
        pair = pair.reshape(fs, -1, pair.shape[-1])
        ob = ob.reshape(fs, -1, ob.shape[-1])
        f32 = jnp.float32
        shapes = (
            *(jax.ShapeDtypeStruct(w.shape, f32) for w in weights),
            *(jax.ShapeDtypeStruct(w.shape, w.dtype) for w in wholes),
            *(jax.ShapeDtypeStruct(m.shape, f32) for m in means),
            *(jax.ShapeDtypeStruct(m.shape, f32) for m in olds),
        )
        vmem = pl.BlockSpec(memory_space=pltpu.VMEM)
        return pl.pallas_call(
            functools.partial(last_kernel, entries),
            out_shape=shapes,
            in_specs=[vmem] * 9,
            out_specs=(pl.BlockSpec(memory_space=pl.ANY),) * 12,
            scratch_shapes=[
                *(pltpu.VMEM(s.shape, s.dtype) for s in shapes[:6]),
                pltpu.SemaphoreType.DMA((9 + 3 * fs,)),
            ],
            compiler_params=pltpu.CompilerParams(vmem_limit_bytes=VMEM_LAST),
        )(*wholes, pair, ob, firsts, seconds, dirs, squares)

    return local


def solution(mesh):
    rows, split_both, columns = P("fs", None), P("fs", "tp"), P(None, "tp")
    in_specs = (rows,) * 2 + (split_both,) * 6 + (rows,) * 3 + (columns,) * 6
    out_specs = (split_both,) * 3 + (columns,) * 9
    return jax.shard_map(
        body(mesh.shape["fs"], mesh.shape["tp"]),
        mesh=mesh,
        in_specs=in_specs,
        out_specs=out_specs,
        check_vma=False,
    )
```

```python
import functools

import jax
import jax.numpy as jnp
from jax import lax
from jax.experimental import pallas as pl
from jax.experimental.pallas import tpu as pltpu
from jax.sharding import PartitionSpec as P

beta_first = 0.8
beta_second = 0.9
floor_mean = 0.005
learn_rate = 0.05

MESH = pl.DeviceIdType.MESH
LINE_SHARE = 8 / 16
BASE_LINES = (0, 1)


def matmul(left, right):
    return jnp.dot(left, right, preferred_element_type=jnp.float32)


def moments(projected, mean_old, square_old):
    moment_one = beta_first * mean_old + (1.0 - beta_first) * projected
    moment_two = beta_second * square_old + (1.0 - beta_second) * projected * projected
    return (moment_one, moment_two, moment_one / jnp.sqrt(moment_two))


def aligned(start, size):
    return pl.ds(pl.multiple_of(start, size), size)


class Gather:
    def __init__(self, fs, me, refs, chunks, lines, piece, several, sems):
        self.fs, self.me, self.refs, self.chunks = fs, me, refs, chunks
        self.lines, self.piece, self.several = lines, piece, several
        self.send_sem, self.step_sem, self.last_sem = sems
        self.relayed = fs == 8
        self.place, self.side = me // 2, lax.rem(me, 2)

    def index(self, step, other=False):
        place = lax.rem(self.place + step + 4, 4)
        return place * 2 + (1 - self.side if other else self.side)

    def arrival(self, w, i, role):
        if self.relayed and role < 6:
            return self.step_sem.at[w, (0, 2, 3, 1, 2, 3)[role], i]
        return self.last_sem.at[w, role - 6 if self.relayed else role]

    def copy(self, w, i, origin, site, role, target):
        return remote(
            self.piece(w, origin, i),
            self.piece(w, origin, i),
            self.send_sem.at[w, site],
            self.arrival(w, i, role),
            fs=target,
        )

    def total(self, w, origin, count, site, role):
        return remote(
            self.several(w, origin, count),
            self.several(w, origin, count),
            self.send_sem.at[w, site],
            self.arrival(w, 0, role),
            fs=lax.rem(self.me + 1, self.fs),
        )

    def arrive(self, w, i, origin, role, inside):
        copy = self.copy(w, i, origin, 0, role, lax.rem(self.me + 1, self.fs))
        pl.when(inside)(copy.wait_recv)

    def sites(self, w, i):
        p = self.place
        line = i < self.lines[w]
        cross = self.index(0, True)
        out = {
            0: (self.me, 0, self.index(1), p < 3),
            1: (self.me, 3, self.index(-1), p > 0),
            2: (self.me, 6, cross, None),
            13: (cross, 7, self.index(1), (p < 3) & (line | (p == 0))),
            14: (cross, 10, self.index(-1), (p > 0) & (line | (p == 3))),
        }
        for d in (1, 2):
            out[2 + d] = (self.index(-d), d, self.index(1), (p >= d) & (p < 3))
            out[4 + d] = (self.index(d), 3 + d, self.index(-1), (p + d < 4) & (p > 0))
        for d in (1, 2, 3):
            below, above = p >= d, p + d < 4
            if d == 1:
                below = below & jnp.logical_not(line | (p == 1))
                above = above & jnp.logical_not(line | (p == 2))
            out[6 + d] = (self.index(-d), 6 + d, cross, below)
            out[9 + d] = (self.index(d), 9 + d, cross, above)
        return out

    def direct(self):
        return [(k - 1, lax.rem(self.me + k, self.fs)) for k in range(1, self.fs)]

    def send(self, w, i, wanted, also=None):
        table = self.sites(w, i)
        for site in wanted:
            origin, role, target, inside = table[site]
            copy = self.copy(w, i, origin, site, role, target)
            if also is not None:
                inside = inside & also
            if inside is None:
                copy.start()
            else:
                pl.when(inside)(copy.start)

    def each(self, step, low=0, high=None):
        high = self.chunks if high is None else high

        def chunk(i, carry):
            for w in range(len(self.refs)):
                step(w, i)
            return carry

        if high - low == 1:
            chunk(low, 0)
        elif high > low:
            lax.fori_loop(low, high, chunk, 0)

    def start(self, low=0, high=None):
        def step(w, i):
            if self.relayed:
                self.send(w, i, (0, 1, 2))
            else:
                for number, target in self.direct():
                    self.copy(w, i, self.me, number, number, target).start()

        self.each(step, low, high)

    def relay_out(self, low=0, high=None):
        p = self.place

        def step(w, i):
            self.arrive(w, i, self.index(-1), 0, p >= 2)
            self.send(w, i, (3, 7), p >= 2)
            self.arrive(w, i, self.index(1), 3, p <= 1)
            self.send(w, i, (5, 10), p <= 1)

        if self.relayed:
            self.each(step, low, high)

    def relay_in(self, low=0, high=None):
        p = self.place

        def step(w, i):
            self.arrive(w, i, self.index(-1), 0, p == 1)
            self.send(w, i, (3,), p == 1)
            self.arrive(w, i, self.index(1), 3, p == 2)
            self.send(w, i, (5,), p == 2)

        if self.relayed:
            self.each(step, low, high)

    def relay(self, d, low=0, high=None):
        p = self.place

        def step(w, i):
            self.arrive(w, i, self.index(-d), d - 1, p >= d)
            self.send(w, i, (2 + d, 6 + d) if d < 3 else (6 + d,))
            self.arrive(w, i, self.index(d), 2 + d, p + d < 4)
            self.send(w, i, (4 + d, 9 + d) if d < 3 else (9 + d,))

        if self.relayed:
            self.each(step, low, high)

    def relay_cross(self):
        if not self.relayed:
            return
        for w in range(len(self.refs)):
            self.total(w, self.index(0, True), self.chunks, 0, 6).wait_recv()
        self.each(lambda w, i: self.send(w, i, (13, 14)))

    def finish(self):
        p = self.place
        for w in range(len(self.refs)):
            if not self.relayed:
                for k in range(1, self.fs):
                    source = lax.rem(self.me + self.fs - k, self.fs)
                    self.total(w, source, self.chunks, 0, k - 1).wait_recv()
                continue
            for d in (1, 2, 3):
                below = self.total(w, self.index(-d, True), self.chunks, 0, 6 + d)
                above = self.total(w, self.index(d, True), self.chunks, 0, 9 + d)
                pl.when(p >= d)(below.wait_recv)
                pl.when(p + d < 4)(above.wait_recv)

    def drain(self):
        p = self.place
        for w in range(len(self.refs)):
            if not self.relayed:
                for number, _ in self.direct():
                    self.total(w, self.me, self.chunks, number, 0).wait_send()
                continue
            on_line, rest = self.lines[w], self.chunks - self.lines[w]
            for site, (origin, _, _, inside) in self.sites(w, 0).items():
                waits = [(self.chunks, inside)]
                if site == 7:
                    waits = [(rest, p >= 2)]
                elif site == 10:
                    waits = [(rest, p <= 1)]
                elif site == 13:
                    waits = [(self.chunks, p == 0), (on_line, (p > 0) & (p < 3))]
                elif site == 14:
                    waits = [(self.chunks, p == 3), (on_line, (p > 0) & (p < 3))]
                for count, when in waits:
                    if count == 0:
                        continue
                    copy = self.total(w, origin, count, site, 0)
                    if when is None:
                        copy.wait_send()
                    else:
                        pl.when(when)(copy.wait_send)


def remote(ref_from, ref_to, send, recv, **device):
    return pltpu.make_async_remote_copy(
        src_ref=ref_from,
        dst_ref=ref_to,
        send_sem=send,
        recv_sem=recv,
        device_id=device,
        device_id_type=MESH,
    )


def kernel(
    fs,
    tp,
    owners,
    mixer_hbm,
    cell_hbm,
    qg_hbm,
    vg_hbm,
    og_hbm,
    qb_hbm,
    vb_hbm,
    ob_hbm,
    qw_hbm,
    vw_hbm,
    ow_hbm,
    qm_hbm,
    vm_hbm,
    om_hbm,
    qs_hbm,
    vs_hbm,
    os_hbm,
    w_all,
    pair_all,
    ob_all,
    firsts,
    seconds,
    dirs,
    squares,
    mixer,
    cell,
    qg,
    vg,
    og,
    qw,
    vw,
    ow,
    means,
    olds,
    proj,
    part,
    parts,
    square_own,
    square_in,
    w_send,
    w_step,
    w_last,
    b_send,
    b_step,
    b_last,
    y_send,
    y_recv,
    c_send,
    c_recv,
    sum_send,
    sum_recv,
    back_send,
    back_recv,
    over_send,
    tp_send,
    tp_recv,
    local_sem,
):
    me, column = lax.axis_index("fs"), lax.axis_index("tp")
    rank, width = qm_hbm.shape
    far, core = column // 2, lax.rem(column, 2)
    fars = tp // 2
    own_bases = (pair_all.at[me, far, core], ob_all.at[me, far, core])
    pair_rows, ob_rows = pair_all.shape[3], ob_all.shape[3]
    pair_from = aligned(column * pair_rows, pair_rows)
    ob_from = aligned(column * ob_rows, ob_rows)
    loads = [
        pltpu.make_async_copy(source, target, local_sem.at[i])
        for i, (source, target) in enumerate(
            (
                (qb_hbm.at[pair_from, :], pair_all.at[me, far, core, :, pl.ds(0, rank)]),
                (vb_hbm.at[pair_from, :], pair_all.at[me, far, core, :, pl.ds(rank, rank)]),
                (ob_hbm.at[ob_from, :], own_bases[1]),
                (qw_hbm, qw),
                (vw_hbm, vw),
                (ow_hbm, ow),
                (mixer_hbm, mixer),
                (cell_hbm, cell),
                (qg_hbm, qg),
                (vg_hbm, vg),
                (og_hbm, og),
                (qm_hbm, means.at[:, pl.ds(0, width)]),
                (vm_hbm, means.at[:, pl.ds(width, width)]),
                (om_hbm, means.at[:, pl.ds(2 * width, 2 * width)]),
                (qs_hbm, olds.at[:, pl.ds(0, width)]),
                (vs_hbm, olds.at[:, pl.ds(width, width)]),
                (os_hbm, olds.at[:, pl.ds(2 * width, 2 * width)]),
            )
        )
    ]
    for load in loads:
        load.start()

    barrier = pltpu.get_barrier_semaphore()
    for k in range(1, fs):
        pl.semaphore_signal(
            barrier, inc=1, device_id={"fs": lax.rem(me + k, fs)}, device_id_type=MESH
        )
    for k in range(1, tp):
        pl.semaphore_signal(
            barrier, inc=1, device_id={"tp": lax.rem(column + k, tp)}, device_id_type=MESH
        )
    pl.semaphore_wait(barrier, fs + tp - 2)

    for load in loads[:3]:
        load.wait()
    bases = (pair_all, ob_all)
    sent = []
    parts_of_bases = Gather(
        fs,
        me,
        bases,
        1,
        BASE_LINES,
        lambda w, origin, i: bases[w].at[origin, far, core],
        lambda w, origin, count: bases[w].at[origin, far, core],
        (b_send, b_step, b_last),
    )
    chunks = w_all.shape[1]
    weights = Gather(
        fs,
        me,
        (w_all,),
        chunks,
        (int(LINE_SHARE * chunks),),
        lambda w, origin, i: w_all.at[origin, i],
        lambda w, origin, count: w_all.at[origin, pl.ds(0, count)],
        (w_send, w_step, w_last),
    )
    parts_of_bases.start()
    for load in loads[3:6]:
        load.wait()
    across, spread = w_all.shape[4], ow.shape[1] // w_all.shape[4]
    for n, own in enumerate((qw, vw)):
        w_all[me, :, n] = own[...].astype(jnp.bfloat16).reshape(chunks, -1, across)
    low_rows = w_all.shape[3] // spread
    for h in range(spread):
        piece = ow[:, h * across : (h + 1) * across].astype(jnp.bfloat16)
        w_all[me, :, 2, h * low_rows : (h + 1) * low_rows, :] = piece.reshape(
            chunks, low_rows, across
        )
    weights.start(0, 1)
    part[...] = jnp.zeros_like(part)
    parts_of_bases.relay(1)
    parts_of_bases.relay_cross()
    weights.start(1, 2)
    parts_of_bases.relay(2)
    weights.start(2, 3)
    parts_of_bases.relay(3)
    weights.start(3)
    parts_of_bases.finish()
    for k in range(1, fars):
        for n, whole in enumerate(bases):
            mine = whole.at[:, far, core]
            copy = remote(
                mine,
                mine,
                y_send.at[n, k - 1],
                y_recv.at[n, k - 1],
                tp=lax.rem(far + k, fars) * 2 + core,
            )
            copy.start()
            sent.append(copy)
    weights.relay_out(0, chunks // 2)
    for k in range(1, fars):
        source = lax.rem(far + fars - k, fars)
        for n, whole in enumerate(bases):
            there = whole.at[:, source, core]
            remote(
                there,
                there,
                y_send.at[n, k - 1],
                y_recv.at[n, k - 1],
                tp=lax.rem(far + k, fars) * 2 + core,
            ).wait_recv()
    for n, whole in enumerate(bases):
        mine = whole.at[:, :, core]
        copy = remote(mine, mine, c_send.at[n], c_recv.at[n], tp=far * 2 + 1 - core)
        copy.start()
        sent.append(copy)
    for load in loads[6:]:
        load.wait()
    for n, whole in enumerate(bases):
        there = whole.at[:, :, 1 - core]
        remote(there, there, c_send.at[n], c_recv.at[n], tp=far * 2 + 1 - core).wait_recv()

    tile = 256

    def project(rows, grad):
        turned = jnp.transpose(rows)
        high = turned.astype(jnp.bfloat16)
        low = (turned - high.astype(jnp.float32)).astype(jnp.bfloat16)
        both = matmul(jnp.concatenate([high, low], axis=0), grad)
        return both[:rank] + both[rank:]

    def flat(ref):
        value = ref[...]
        return value.reshape(-1, value.shape[-1])

    def step(t, carry):
        at = aligned(t * tile, tile)
        rows = matmul(mixer[at, :], flat(pair_all))
        part[:, :width] += project(rows[:, :rank], qg[at, :])
        part[:, width : 2 * width] += project(rows[:, rank:], vg[at, :])
        part[:, 2 * width :] += project(matmul(cell[at, :], flat(ob_all)), og[at, :])
        return carry

    lax.fori_loop(0, mixer.shape[0] // tile, step, 0)

    first_owner = (fs - owners) // 2
    share = rank // owners

    def owns(index):
        return (index >= first_owner) & (index < first_owner + owners)

    def strip_of(index):
        return lax.rem(index - first_owner + fs, owners)

    def strip(index):
        return aligned(strip_of(index) * share, share)

    drains = []
    for k in range(1, fs):
        target = lax.rem(me + k, fs)
        copy = remote(
            part.at[strip(target), :],
            parts.at[k - 1],
            sum_send.at[k - 1],
            sum_recv.at[k - 1],
            fs=target,
        )
        pl.when(owns(target))(copy.start)
        drains.append((copy, owns(target)))

    weights.relay_out(chunks // 2)
    weights.relay_in(0, chunks // 4)

    def gram(ref):
        rows, size = ref.shape[3], ref.shape[4]

        def add(i, total):
            piece = ref[i].reshape(-1, size)
            turned = jnp.transpose(piece.astype(jnp.float32)).astype(jnp.bfloat16)
            return total + matmul(turned, piece)

        return lax.fori_loop(0, ref.shape[0], add, jnp.zeros((size, size), jnp.float32))

    gram_pair = gram(pair_all)
    gram_output = gram(ob_all)

    side = lax.rem(me, 2)
    relayed = weights.relayed
    back = []
    for k in range(1, fs):
        target = lax.rem(me + k, fs)
        mine = proj.at[strip(me), :]
        inside = owns(me)
        if relayed:
            inside = inside & (owns(target) | (lax.rem(target, 2) == side))
        copy = remote(
            mine, mine, back_send.at[k - 1], back_recv.at[strip_of(me)], fs=target
        )
        back.append((copy, inside))
    other = me + 1 - 2 * side if relayed else lax.rem(me + 1, fs)
    returned = []
    for j in range(owners):
        there = proj.at[pl.ds(j * share, share), :]
        source = first_owner + j
        straight = me != source
        if relayed:
            same = side == source % 2
            straight = straight & (owns(me) | same)
        over = remote(there, there, over_send.at[j], back_recv.at[j], fs=other)
        returned.append((over, straight, jnp.logical_not(owns(me)) if relayed else None, source % 2))

    @pl.when(owns(me))
    def _():
        for k in range(1, fs):
            remote(
                part.at[strip(me), :],
                parts.at[k - 1],
                sum_send.at[k - 1],
                sum_recv.at[k - 1],
                fs=lax.rem(me + k, fs),
            ).wait_recv()
        total = part[strip(me), :]
        for k in range(1, fs):
            total = total + parts[k - 1]
        proj[strip(me), :] = total.astype(proj.dtype)

    for copy, inside in back:
        pl.when(inside)(copy.start)

    weights.relay_in(chunks // 4)
    weights.relay(2)
    weights.relay_cross()

    for over, straight, at_end, parity in returned:
        pl.when(straight)(over.wait_recv)
        if relayed:
            pl.when(at_end & (side == parity))(over.start)
    weights.relay(3)
    if relayed:
        for over, straight, at_end, parity in returned:
            pl.when(at_end & (side != parity))(over.wait_recv)

    def norm(basis_gram, left, columns):
        at = pl.ds(left, columns)
        first, second, direction = moments(
            proj[:, at].astype(jnp.float32), means[:, at], olds[:, at]
        )
        firsts[:, at] = first
        seconds[:, at] = second
        high = direction.astype(jnp.bfloat16)
        dirs[:rank, at] = high
        dirs[rank:, at] = (direction - high.astype(jnp.float32)).astype(jnp.bfloat16)
        turned = jnp.dot(
            basis_gram,
            direction,
            precision=lax.Precision.HIGHEST,
            preferred_element_type=jnp.float32,
        )
        lanes = jnp.sum(direction * turned, axis=0, keepdims=True)
        return jnp.sum(lanes, axis=1, keepdims=True)

    partial = (
        norm(gram_pair[:rank, :rank], 0, width)
        + norm(gram_pair[rank:, rank:], width, width)
        + norm(gram_output, 2 * width, 2 * width)
    )
    square_own[...] = jnp.broadcast_to(partial, square_own.shape)
    shares = []
    for k in range(1, tp):
        copy = remote(
            square_own,
            square_in.at[k - 1],
            tp_send.at[k - 1],
            tp_recv.at[k - 1],
            tp=lax.rem(column + k, tp),
        )
        copy.start()
        shares.append(copy)

    for copy in shares:
        copy.wait_recv()
    whole_squares = square_own[...]
    for k in range(1, tp):
        whole_squares = whole_squares + square_in[k - 1]
    squares[...] = whole_squares
    weights.finish()
    for copy in sent + shares:
        copy.wait_send()
    for copy, inside in drains + back:
        pl.when(inside)(copy.wait_send)
    if relayed:
        for over, straight, at_end, parity in returned:
            pl.when(at_end & (side == parity))(over.wait_send)
    parts_of_bases.drain()
    weights.drain()


def exchange(fs, tp, mixer, cell, grads, bases, weights, means, olds):
    rank = means[0].shape[0]
    total = sum(grad.shape[1] for grad in grads)
    owners = min(4, fs)
    bf16, f32 = jnp.bfloat16, jnp.float32
    hbm, vmem = pl.BlockSpec(memory_space=pltpu.HBM), pl.BlockSpec(memory_space=pltpu.VMEM)
    dma = pltpu.SemaphoreType.DMA

    rows, across = weights[0].shape
    chunks = min(16, rows * across // (16 * weights[2].shape[1]))

    def parted(array, columns):
        return jax.ShapeDtypeStruct((fs, tp // 2, 2, array.shape[0] // tp, columns), bf16)

    return pl.pallas_call(
        functools.partial(kernel, fs, tp, owners),
        out_shape=(
            jax.ShapeDtypeStruct((fs, chunks, 3, rows // chunks, across), bf16),
            parted(bases[0], 2 * rank),
            parted(bases[2], rank),
            jax.ShapeDtypeStruct((rank, total), f32),
            jax.ShapeDtypeStruct((rank, total), f32),
            jax.ShapeDtypeStruct((2 * rank, total), bf16),
            jax.ShapeDtypeStruct((8, 128), f32),
        ),
        in_specs=[hbm] * 17,
        out_specs=(vmem,) * 7,
        scratch_shapes=[
            *(pltpu.VMEM(array.shape, bf16) for array in (mixer, cell, *grads)),
            *(pltpu.VMEM(array.shape, f32) for array in weights),
            pltpu.VMEM((rank, total), f32),
            pltpu.VMEM((rank, total), f32),
            pltpu.VMEM((rank, total), bf16),
            pltpu.VMEM((rank, total), f32),
            pltpu.VMEM((fs - 1, rank // owners, total), f32),
            pltpu.VMEM((8, 128), f32),
            pltpu.VMEM((tp - 1, 8, 128), f32),
            dma((1, max(15, fs - 1))),
            dma((1, 4, chunks)),
            dma((1, max(7, fs - 1))),
            dma((2, max(15, fs - 1))),
            dma((2, 4, 1)),
            dma((2, max(7, fs - 1))),
            dma((2, max(1, tp // 2 - 1))),
            dma((2, max(1, tp // 2 - 1))),
            dma((2,)),
            dma((2,)),
            dma((fs - 1,)),
            dma((fs - 1,)),
            dma((fs - 1,)),
            dma((owners,)),
            dma((owners,)),
            dma((tp - 1,)),
            dma((tp - 1,)),
            dma((17,)),
        ],
        compiler_params=pltpu.CompilerParams(
            collective_id=0, has_side_effects=True, vmem_limit_bytes=VMEM_MAIN
        ),
    )(*(pltpu.with_memory_space_constraint(a, pltpu.HBM) for a in (mixer, cell, *grads, *bases, *weights, *means, *olds)))


VMEM_MAIN = 30 * 1024 * 1024
VMEM_LAST = 24 * 1024 * 1024


def last_kernel(entries, *refs):
    w_all, pair, ob, firsts, seconds, dirs, squares = refs[:7]
    outputs, stage, sem = refs[7:19], refs[19:25], refs[25]
    rank, across = pair.shape[2] // 2, w_all.shape[4]
    me = lax.axis_index("fs")
    copies = []

    def put(source, target):
        copy = pltpu.make_async_copy(source, target, sem.at[len(copies)])
        copy.start()
        copies.append(copy)

    cuts, left = [], 0
    for output in outputs[:3]:
        cuts.append((left, output.shape[1]))
        left += output.shape[1]
    for n, cut in enumerate(cuts):
        put(firsts.at[:, pl.ds(*cut)], outputs[6 + n])
        put(seconds.at[:, pl.ds(*cut)], outputs[9 + n])
    factor = 1.0 / jnp.sqrt(squares[0:1, 0:1] / entries + floor_mean)
    scale = -learn_rate * factor
    bases = ((pair, 0), (pair, rank), (ob, 0))
    for n, (cut, (base, low)) in enumerate(zip(cuts, bases)):
        both = dirs[:, pl.ds(*cut)]
        own = base[me, :, low : low + rank]
        stage[n][...] = -factor * matmul(jnp.concatenate([own, own], axis=1), both)
        put(stage[n], outputs[n])
        block = base.shape[1]
        rows = block // w_all.shape[1]
        for o in range(base.shape[0]):
            update = scale * matmul(base[o, :, low : low + rank], both[:rank])
            for h in range(cut[1] // across):
                held = w_all[o, :, n, h * rows : (h + 1) * rows, :].reshape(block, across)
                stage[3 + n][pl.ds(o * block, block), h * across : (h + 1) * across] = (
                    held.astype(jnp.float32) + update[:, h * across : (h + 1) * across]
                ).astype(jnp.bfloat16)
            at = pl.ds(o * block, block)
            put(stage[3 + n].at[at, :], outputs[3 + n].at[at, :])
    for copy in copies:
        copy.wait()


def body(fs, tp):
    def local(
        mixer_input,
        cell_output,
        query_grad,
        value_grad,
        output_grad,
        query_weight,
        value_weight,
        output_weight,
        query_basis,
        value_basis,
        output_basis,
        query_mean,
        value_mean,
        output_mean,
        query_square,
        value_square,
        output_square,
    ):
        means = (query_mean, value_mean, output_mean)
        olds = (query_square, value_square, output_square)
        weights = (query_weight, value_weight, output_weight)
        w_all, pair, ob, *rest = exchange(
            fs,
            tp,
            mixer_input,
            cell_output,
            (query_grad, value_grad, output_grad),
            (query_basis, value_basis, output_basis),
            weights,
            means,
            olds,
        )
        entries = float(sum(w.shape[0] * fs * w.shape[1] * tp for w in weights))
        pair = pair.reshape(fs, -1, pair.shape[-1])
        ob = ob.reshape(fs, -1, ob.shape[-1])
        f32 = jnp.float32
        shapes = (
            *(jax.ShapeDtypeStruct(w.shape, f32) for w in weights),
            *(jax.ShapeDtypeStruct((w.shape[0] * fs, w.shape[1]), jnp.bfloat16) for w in weights),
            *(jax.ShapeDtypeStruct(m.shape, f32) for m in means),
            *(jax.ShapeDtypeStruct(m.shape, f32) for m in olds),
        )
        vmem = pl.BlockSpec(memory_space=pltpu.VMEM)
        return pl.pallas_call(
            functools.partial(last_kernel, entries),
            out_shape=shapes,
            in_specs=[vmem] * 7,
            out_specs=(pl.BlockSpec(memory_space=pl.ANY),) * 12,
            scratch_shapes=[
                *(pltpu.VMEM(s.shape, s.dtype) for s in shapes[:6]),
                pltpu.SemaphoreType.DMA((9 + 3 * fs,)),
            ],
            compiler_params=pltpu.CompilerParams(vmem_limit_bytes=VMEM_LAST),
        )(w_all, pair, ob, *rest)

    return local


def solution(mesh):
    rows, split_both, columns = P("fs", None), P("fs", "tp"), P(None, "tp")
    in_specs = (rows,) * 2 + (split_both,) * 6 + (rows,) * 3 + (columns,) * 6
    out_specs = (split_both,) * 3 + (columns,) * 9
    return jax.shard_map(
        body(mesh.shape["fs"], mesh.shape["tp"]),
        mesh=mesh,
        in_specs=in_specs,
        out_specs=out_specs,
        check_vma=False,
    )
```

```python
import functools

import jax
import jax.numpy as jnp
from jax import lax
from jax.experimental import pallas as pl
from jax.experimental.pallas import tpu as pltpu
from jax.sharding import PartitionSpec as P

beta_first = 0.8
beta_second = 0.9
floor_mean = 0.005
learn_rate = 0.05

MESH = pl.DeviceIdType.MESH
LINE_SHARE = 8 / 16
BASE_LINES = (0, 1)


def matmul(left, right):
    return jnp.dot(left, right, preferred_element_type=jnp.float32)


def moments(projected, mean_old, square_old):
    moment_one = beta_first * mean_old + (1.0 - beta_first) * projected
    moment_two = beta_second * square_old + (1.0 - beta_second) * projected * projected
    return (moment_one, moment_two, moment_one / jnp.sqrt(moment_two))


def aligned(start, size):
    return pl.ds(pl.multiple_of(start, size), size)


class Gather:
    def __init__(self, fs, me, refs, chunks, lines, piece, several, sems):
        self.fs, self.me, self.refs, self.chunks = fs, me, refs, chunks
        self.lines, self.piece, self.several = lines, piece, several
        self.send_sem, self.step_sem, self.last_sem = sems
        self.relayed = fs == 8
        self.place, self.side = me // 2, lax.rem(me, 2)

    def index(self, step, other=False):
        place = lax.rem(self.place + step + 4, 4)
        return place * 2 + (1 - self.side if other else self.side)

    def arrival(self, w, i, role):
        if self.relayed and role < 6:
            return self.step_sem.at[w, (0, 2, 3, 1, 2, 3)[role], i]
        return self.last_sem.at[w, role - 6 if self.relayed else role]

    def copy(self, w, i, origin, site, role, target):
        return remote(
            self.piece(w, origin, i),
            self.piece(w, origin, i),
            self.send_sem.at[w, site],
            self.arrival(w, i, role),
            fs=target,
        )

    def total(self, w, origin, count, site, role):
        return remote(
            self.several(w, origin, count),
            self.several(w, origin, count),
            self.send_sem.at[w, site],
            self.arrival(w, 0, role),
            fs=lax.rem(self.me + 1, self.fs),
        )

    def arrive(self, w, i, origin, role, inside):
        copy = self.copy(w, i, origin, 0, role, lax.rem(self.me + 1, self.fs))
        pl.when(inside)(copy.wait_recv)

    def sites(self, w, i):
        p = self.place
        line = i < self.lines[w]
        cross = self.index(0, True)
        out = {
            0: (self.me, 0, self.index(1), p < 3),
            1: (self.me, 3, self.index(-1), p > 0),
            2: (self.me, 6, cross, None),
            13: (cross, 7, self.index(1), (p < 3) & (line | (p == 0))),
            14: (cross, 10, self.index(-1), (p > 0) & (line | (p == 3))),
        }
        for d in (1, 2):
            out[2 + d] = (self.index(-d), d, self.index(1), (p >= d) & (p < 3))
            out[4 + d] = (self.index(d), 3 + d, self.index(-1), (p + d < 4) & (p > 0))
        for d in (1, 2, 3):
            below, above = p >= d, p + d < 4
            if d == 1:
                below = below & jnp.logical_not(line | (p == 1))
                above = above & jnp.logical_not(line | (p == 2))
            out[6 + d] = (self.index(-d), 6 + d, cross, below)
            out[9 + d] = (self.index(d), 9 + d, cross, above)
        return out

    def direct(self):
        return [(k - 1, lax.rem(self.me + k, self.fs)) for k in range(1, self.fs)]

    def send(self, w, i, wanted, also=None):
        table = self.sites(w, i)
        for site in wanted:
            origin, role, target, inside = table[site]
            copy = self.copy(w, i, origin, site, role, target)
            if also is not None:
                inside = inside & also
            if inside is None:
                copy.start()
            else:
                pl.when(inside)(copy.start)

    def each(self, step, low=0, high=None):
        high = self.chunks if high is None else high

        def chunk(i, carry):
            for w in range(len(self.refs)):
                step(w, i)
            return carry

        if high - low == 1:
            chunk(low, 0)
        elif high > low:
            lax.fori_loop(low, high, chunk, 0)

    def start(self, low=0, high=None):
        def step(w, i):
            if self.relayed:
                self.send(w, i, (0, 1, 2))
            else:
                for number, target in self.direct():
                    self.copy(w, i, self.me, number, number, target).start()

        self.each(step, low, high)

    def relay_out(self, low=0, high=None):
        p = self.place

        def step(w, i):
            self.arrive(w, i, self.index(-1), 0, p >= 2)
            self.send(w, i, (3, 7), p >= 2)
            self.arrive(w, i, self.index(1), 3, p <= 1)
            self.send(w, i, (5, 10), p <= 1)

        if self.relayed:
            self.each(step, low, high)

    def relay_in(self, low=0, high=None):
        p = self.place

        def step(w, i):
            self.arrive(w, i, self.index(-1), 0, p == 1)
            self.send(w, i, (3,), p == 1)
            self.arrive(w, i, self.index(1), 3, p == 2)
            self.send(w, i, (5,), p == 2)

        if self.relayed:
            self.each(step, low, high)

    def relay(self, d, low=0, high=None):
        p = self.place

        def step(w, i):
            self.arrive(w, i, self.index(-d), d - 1, p >= d)
            self.send(w, i, (2 + d, 6 + d) if d < 3 else (6 + d,))
            self.arrive(w, i, self.index(d), 2 + d, p + d < 4)
            self.send(w, i, (4 + d, 9 + d) if d < 3 else (9 + d,))

        if self.relayed:
            self.each(step, low, high)

    def relay_cross(self):
        if not self.relayed:
            return
        for w in range(len(self.refs)):
            self.total(w, self.index(0, True), self.chunks, 0, 6).wait_recv()
        self.each(lambda w, i: self.send(w, i, (13, 14)))

    def finish(self):
        p = self.place
        for w in range(len(self.refs)):
            if not self.relayed:
                for k in range(1, self.fs):
                    source = lax.rem(self.me + self.fs - k, self.fs)
                    self.total(w, source, self.chunks, 0, k - 1).wait_recv()
                continue
            for d in (1, 2, 3):
                below = self.total(w, self.index(-d, True), self.chunks, 0, 6 + d)
                above = self.total(w, self.index(d, True), self.chunks, 0, 9 + d)
                pl.when(p >= d)(below.wait_recv)
                pl.when(p + d < 4)(above.wait_recv)

    def drain(self):
        p = self.place
        for w in range(len(self.refs)):
            if not self.relayed:
                for number, _ in self.direct():
                    self.total(w, self.me, self.chunks, number, 0).wait_send()
                continue
            on_line, rest = self.lines[w], self.chunks - self.lines[w]
            for site, (origin, _, _, inside) in self.sites(w, 0).items():
                waits = [(self.chunks, inside)]
                if site == 7:
                    waits = [(rest, p >= 2)]
                elif site == 10:
                    waits = [(rest, p <= 1)]
                elif site == 13:
                    waits = [(self.chunks, p == 0), (on_line, (p > 0) & (p < 3))]
                elif site == 14:
                    waits = [(self.chunks, p == 3), (on_line, (p > 0) & (p < 3))]
                for count, when in waits:
                    if count == 0:
                        continue
                    copy = self.total(w, origin, count, site, 0)
                    if when is None:
                        copy.wait_send()
                    else:
                        pl.when(when)(copy.wait_send)


def remote(ref_from, ref_to, send, recv, **device):
    return pltpu.make_async_remote_copy(
        src_ref=ref_from,
        dst_ref=ref_to,
        send_sem=send,
        recv_sem=recv,
        device_id=device,
        device_id_type=MESH,
    )


def kernel(
    fs,
    tp,
    owners,
    mixer_hbm,
    cell_hbm,
    qg_hbm,
    vg_hbm,
    og_hbm,
    qb_hbm,
    vb_hbm,
    ob_hbm,
    qw_hbm,
    vw_hbm,
    ow_hbm,
    qm_hbm,
    vm_hbm,
    om_hbm,
    qs_hbm,
    vs_hbm,
    os_hbm,
    w_all,
    pair_all,
    ob_all,
    firsts,
    seconds,
    dirs,
    squares,
    mixer,
    cell,
    qg,
    vg,
    og,
    qw,
    vw,
    ow,
    means,
    olds,
    proj,
    part,
    parts,
    square_own,
    square_in,
    w_send,
    w_step,
    w_last,
    b_send,
    b_step,
    b_last,
    y_send,
    y_recv,
    c_send,
    c_recv,
    sum_send,
    sum_recv,
    back_send,
    back_recv,
    over_send,
    tp_send,
    tp_recv,
    local_sem,
):
    me, column = lax.axis_index("fs"), lax.axis_index("tp")
    rank, width = qm_hbm.shape
    far, core = column // 2, lax.rem(column, 2)
    fars = tp // 2
    own_bases = (pair_all.at[me, far, core], ob_all.at[me, far, core])
    pair_rows, ob_rows = pair_all.shape[3], ob_all.shape[3]
    pair_from = aligned(column * pair_rows, pair_rows)
    ob_from = aligned(column * ob_rows, ob_rows)
    loads = [
        pltpu.make_async_copy(source, target, local_sem.at[i])
        for i, (source, target) in enumerate(
            (
                (qb_hbm.at[pair_from, :], pair_all.at[me, far, core, :, pl.ds(0, rank)]),
                (vb_hbm.at[pair_from, :], pair_all.at[me, far, core, :, pl.ds(rank, rank)]),
                (ob_hbm.at[ob_from, :], own_bases[1]),
                (qw_hbm, qw),
                (vw_hbm, vw),
                (ow_hbm, ow),
                (mixer_hbm, mixer),
                (cell_hbm, cell),
                (qg_hbm, qg),
                (vg_hbm, vg),
                (og_hbm, og),
                (qm_hbm, means.at[:, pl.ds(0, width)]),
                (vm_hbm, means.at[:, pl.ds(width, width)]),
                (om_hbm, means.at[:, pl.ds(2 * width, 2 * width)]),
                (qs_hbm, olds.at[:, pl.ds(0, width)]),
                (vs_hbm, olds.at[:, pl.ds(width, width)]),
                (os_hbm, olds.at[:, pl.ds(2 * width, 2 * width)]),
            )
        )
    ]
    for load in loads:
        load.start()

    barrier = pltpu.get_barrier_semaphore()

    def greet(target):
        pl.semaphore_signal(
            barrier, inc=1, device_id={"fs": target}, device_id_type=MESH
        )

    place = me // 2
    for k in range(1, tp):
        pl.semaphore_signal(
            barrier, inc=1, device_id={"tp": lax.rem(column + k, tp)}, device_id_type=MESH
        )
    if fs == 8:
        greet(me + 1 - 2 * lax.rem(me, 2))
        pl.when(place < 3)(lambda: greet(lax.rem(me + 2, fs)))
        pl.when(place > 0)(lambda: greet(lax.rem(me + fs - 2, fs)))
        inner = (place > 0) & (place < 3)
        pl.when(inner)(lambda: pl.semaphore_wait(barrier, tp + 2))
        pl.when(jnp.logical_not(inner))(lambda: pl.semaphore_wait(barrier, tp + 1))
    else:
        for k in range(1, fs):
            greet(lax.rem(me + k, fs))
        pl.semaphore_wait(barrier, fs + tp - 2)

    for load in loads[:3]:
        load.wait()
    bases = (pair_all, ob_all)
    sent = []
    parts_of_bases = Gather(
        fs,
        me,
        bases,
        1,
        BASE_LINES,
        lambda w, origin, i: bases[w].at[origin, far, core],
        lambda w, origin, count: bases[w].at[origin, far, core],
        (b_send, b_step, b_last),
    )
    chunks = w_all.shape[1]
    weights = Gather(
        fs,
        me,
        (w_all,),
        chunks,
        (int(LINE_SHARE * chunks),),
        lambda w, origin, i: w_all.at[origin, i],
        lambda w, origin, count: w_all.at[origin, pl.ds(0, count)],
        (w_send, w_step, w_last),
    )
    parts_of_bases.start()
    for load in loads[3:6]:
        load.wait()
    across, spread = w_all.shape[4], ow.shape[1] // w_all.shape[4]
    for n, own in enumerate((qw, vw)):
        w_all[me, :, n] = own[...].astype(jnp.bfloat16).reshape(chunks, -1, across)
    low_rows = w_all.shape[3] // spread
    for h in range(spread):
        piece = ow[:, h * across : (h + 1) * across].astype(jnp.bfloat16)
        w_all[me, :, 2, h * low_rows : (h + 1) * low_rows, :] = piece.reshape(
            chunks, low_rows, across
        )
    weights.start(0, 1)
    part[...] = jnp.zeros_like(part)
    parts_of_bases.relay(1)
    parts_of_bases.relay_cross()
    weights.start(1, 2)
    parts_of_bases.relay(2)
    weights.start(2, 3)
    parts_of_bases.relay(3)
    weights.start(3)
    parts_of_bases.finish()
    for k in range(1, fars):
        for n, whole in enumerate(bases):
            mine = whole.at[:, far, core]
            copy = remote(
                mine,
                mine,
                y_send.at[n, k - 1],
                y_recv.at[n, k - 1],
                tp=lax.rem(far + k, fars) * 2 + core,
            )
            copy.start()
            sent.append(copy)
    weights.relay_out(0, chunks // 2)
    for k in range(1, fars):
        source = lax.rem(far + fars - k, fars)
        for n, whole in enumerate(bases):
            there = whole.at[:, source, core]
            remote(
                there,
                there,
                y_send.at[n, k - 1],
                y_recv.at[n, k - 1],
                tp=lax.rem(far + k, fars) * 2 + core,
            ).wait_recv()
    for n, whole in enumerate(bases):
        mine = whole.at[:, :, core]
        copy = remote(mine, mine, c_send.at[n], c_recv.at[n], tp=far * 2 + 1 - core)
        copy.start()
        sent.append(copy)
    for load in loads[6:]:
        load.wait()
    for n, whole in enumerate(bases):
        there = whole.at[:, :, 1 - core]
        remote(there, there, c_send.at[n], c_recv.at[n], tp=far * 2 + 1 - core).wait_recv()

    tile = 256

    def project(rows, grad):
        turned = jnp.transpose(rows)
        high = turned.astype(jnp.bfloat16)
        low = (turned - high.astype(jnp.float32)).astype(jnp.bfloat16)
        both = matmul(jnp.concatenate([high, low], axis=0), grad)
        return both[:rank] + both[rank:]

    def flat(ref):
        value = ref[...]
        return value.reshape(-1, value.shape[-1])

    def step(t, carry):
        at = aligned(t * tile, tile)
        rows = matmul(mixer[at, :], flat(pair_all))
        part[:, :width] += project(rows[:, :rank], qg[at, :])
        part[:, width : 2 * width] += project(rows[:, rank:], vg[at, :])
        part[:, 2 * width :] += project(matmul(cell[at, :], flat(ob_all)), og[at, :])
        return carry

    lax.fori_loop(0, mixer.shape[0] // tile, step, 0)

    first_owner = (fs - owners) // 2
    share = rank // owners

    def owns(index):
        return (index >= first_owner) & (index < first_owner + owners)

    def strip_of(index):
        return lax.rem(index - first_owner + fs, owners)

    def strip(index):
        return aligned(strip_of(index) * share, share)

    drains = []
    for k in range(1, fs):
        target = lax.rem(me + k, fs)
        copy = remote(
            part.at[strip(target), :],
            parts.at[k - 1],
            sum_send.at[k - 1],
            sum_recv.at[k - 1],
            fs=target,
        )
        pl.when(owns(target))(copy.start)
        drains.append((copy, owns(target)))

    weights.relay_out(chunks // 2)
    weights.relay_in(0, chunks // 4)

    def gram(ref):
        rows, size = ref.shape[3], ref.shape[4]

        def add(i, total):
            piece = ref[i].reshape(-1, size)
            turned = jnp.transpose(piece.astype(jnp.float32)).astype(jnp.bfloat16)
            return total + matmul(turned, piece)

        return lax.fori_loop(0, ref.shape[0], add, jnp.zeros((size, size), jnp.float32))

    gram_pair = gram(pair_all)
    gram_output = gram(ob_all)

    side = lax.rem(me, 2)
    relayed = weights.relayed
    back = []
    for k in range(1, fs):
        target = lax.rem(me + k, fs)
        mine = proj.at[strip(me), :]
        inside = owns(me)
        if relayed:
            inside = inside & (owns(target) | (lax.rem(target, 2) == side))
        copy = remote(
            mine, mine, back_send.at[k - 1], back_recv.at[strip_of(me)], fs=target
        )
        back.append((copy, inside))
    other = me + 1 - 2 * side if relayed else lax.rem(me + 1, fs)
    returned = []
    for j in range(owners):
        there = proj.at[pl.ds(j * share, share), :]
        source = first_owner + j
        straight = me != source
        if relayed:
            same = side == source % 2
            straight = straight & (owns(me) | same)
        over = remote(there, there, over_send.at[j], back_recv.at[j], fs=other)
        returned.append((over, straight, jnp.logical_not(owns(me)) if relayed else None, source % 2))

    @pl.when(owns(me))
    def _():
        for k in range(1, fs):
            remote(
                part.at[strip(me), :],
                parts.at[k - 1],
                sum_send.at[k - 1],
                sum_recv.at[k - 1],
                fs=lax.rem(me + k, fs),
            ).wait_recv()
        total = part[strip(me), :]
        for k in range(1, fs):
            total = total + parts[k - 1]
        proj[strip(me), :] = total.astype(proj.dtype)

    for copy, inside in back:
        pl.when(inside)(copy.start)

    weights.relay_in(chunks // 4)
    weights.relay(2)
    weights.relay_cross()

    for over, straight, at_end, parity in returned:
        pl.when(straight)(over.wait_recv)
        if relayed:
            pl.when(at_end & (side == parity))(over.start)
    weights.relay(3)
    if relayed:
        for over, straight, at_end, parity in returned:
            pl.when(at_end & (side != parity))(over.wait_recv)

    def norm(basis_gram, left, columns):
        at = pl.ds(left, columns)
        first, second, direction = moments(
            proj[:, at].astype(jnp.float32), means[:, at], olds[:, at]
        )
        firsts[:, at] = first
        seconds[:, at] = second
        high = direction.astype(jnp.bfloat16)
        dirs[:rank, at] = high
        dirs[rank:, at] = (direction - high.astype(jnp.float32)).astype(jnp.bfloat16)
        turned = jnp.dot(
            basis_gram,
            direction,
            precision=lax.Precision.HIGHEST,
            preferred_element_type=jnp.float32,
        )
        lanes = jnp.sum(direction * turned, axis=0, keepdims=True)
        return jnp.sum(lanes, axis=1, keepdims=True)

    partial = (
        norm(gram_pair[:rank, :rank], 0, width)
        + norm(gram_pair[rank:, rank:], width, width)
        + norm(gram_output, 2 * width, 2 * width)
    )
    square_own[...] = jnp.broadcast_to(partial, square_own.shape)
    shares = []
    for k in range(1, tp):
        copy = remote(
            square_own,
            square_in.at[k - 1],
            tp_send.at[k - 1],
            tp_recv.at[k - 1],
            tp=lax.rem(column + k, tp),
        )
        copy.start()
        shares.append(copy)

    for copy in shares:
        copy.wait_recv()
    whole_squares = square_own[...]
    for k in range(1, tp):
        whole_squares = whole_squares + square_in[k - 1]
    squares[...] = whole_squares
    weights.finish()
    for copy in sent + shares:
        copy.wait_send()
    for copy, inside in drains + back:
        pl.when(inside)(copy.wait_send)
    if relayed:
        for over, straight, at_end, parity in returned:
            pl.when(at_end & (side == parity))(over.wait_send)
    parts_of_bases.drain()
    weights.drain()


def exchange(fs, tp, mixer, cell, grads, bases, weights, means, olds):
    rank = means[0].shape[0]
    total = sum(grad.shape[1] for grad in grads)
    owners = min(4, fs)
    bf16, f32 = jnp.bfloat16, jnp.float32
    hbm, vmem = pl.BlockSpec(memory_space=pltpu.HBM), pl.BlockSpec(memory_space=pltpu.VMEM)
    dma = pltpu.SemaphoreType.DMA

    rows, across = weights[0].shape
    chunks = min(16, rows * across // (16 * weights[2].shape[1]))

    def parted(array, columns):
        return jax.ShapeDtypeStruct((fs, tp // 2, 2, array.shape[0] // tp, columns), bf16)

    return pl.pallas_call(
        functools.partial(kernel, fs, tp, owners),
        out_shape=(
            jax.ShapeDtypeStruct((fs, chunks, 3, rows // chunks, across), bf16),
            parted(bases[0], 2 * rank),
            parted(bases[2], rank),
            jax.ShapeDtypeStruct((rank, total), f32),
            jax.ShapeDtypeStruct((rank, total), f32),
            jax.ShapeDtypeStruct((2 * rank, total), bf16),
            jax.ShapeDtypeStruct((8, 128), f32),
        ),
        in_specs=[hbm] * 17,
        out_specs=(vmem,) * 7,
        scratch_shapes=[
            *(pltpu.VMEM(array.shape, bf16) for array in (mixer, cell, *grads)),
            *(pltpu.VMEM(array.shape, f32) for array in weights),
            pltpu.VMEM((rank, total), f32),
            pltpu.VMEM((rank, total), f32),
            pltpu.VMEM((rank, total), bf16),
            pltpu.VMEM((rank, total), f32),
            pltpu.VMEM((fs - 1, rank // owners, total), f32),
            pltpu.VMEM((8, 128), f32),
            pltpu.VMEM((tp - 1, 8, 128), f32),
            dma((1, max(15, fs - 1))),
            dma((1, 4, chunks)),
            dma((1, max(7, fs - 1))),
            dma((2, max(15, fs - 1))),
            dma((2, 4, 1)),
            dma((2, max(7, fs - 1))),
            dma((2, max(1, tp // 2 - 1))),
            dma((2, max(1, tp // 2 - 1))),
            dma((2,)),
            dma((2,)),
            dma((fs - 1,)),
            dma((fs - 1,)),
            dma((fs - 1,)),
            dma((owners,)),
            dma((owners,)),
            dma((tp - 1,)),
            dma((tp - 1,)),
            dma((17,)),
        ],
        compiler_params=pltpu.CompilerParams(
            collective_id=0, has_side_effects=True, vmem_limit_bytes=VMEM_MAIN
        ),
    )(*(pltpu.with_memory_space_constraint(a, pltpu.HBM) for a in (mixer, cell, *grads, *bases, *weights, *means, *olds)))


VMEM_MAIN = 30 * 1024 * 1024
VMEM_LAST = 24 * 1024 * 1024


def last_kernel(entries, *refs):
    w_all, pair, ob, firsts, seconds, dirs, squares = refs[:7]
    outputs, stage, sem = refs[7:19], refs[19:25], refs[25]
    rank, across = pair.shape[2] // 2, w_all.shape[4]
    me = lax.axis_index("fs")
    copies = []

    def put(source, target):
        copy = pltpu.make_async_copy(source, target, sem.at[len(copies)])
        copy.start()
        copies.append(copy)

    cuts, left = [], 0
    for output in outputs[:3]:
        cuts.append((left, output.shape[1]))
        left += output.shape[1]
    for n, cut in enumerate(cuts):
        put(firsts.at[:, pl.ds(*cut)], outputs[6 + n])
        put(seconds.at[:, pl.ds(*cut)], outputs[9 + n])
    factor = 1.0 / jnp.sqrt(squares[0:1, 0:1] / entries + floor_mean)
    scale = -learn_rate * factor
    bases = ((pair, 0), (pair, rank), (ob, 0))
    for n, (cut, (base, low)) in enumerate(zip(cuts, bases)):
        both = dirs[:, pl.ds(*cut)]
        own = base[me, :, low : low + rank]
        stage[n][...] = -factor * matmul(jnp.concatenate([own, own], axis=1), both)
        put(stage[n], outputs[n])
        block = base.shape[1]
        rows = block // w_all.shape[1]
        for o in range(base.shape[0]):
            update = scale * matmul(base[o, :, low : low + rank], both[:rank])
            for h in range(cut[1] // across):
                held = w_all[o, :, n, h * rows : (h + 1) * rows, :].reshape(block, across)
                stage[3 + n][pl.ds(o * block, block), h * across : (h + 1) * across] = (
                    held.astype(jnp.float32) + update[:, h * across : (h + 1) * across]
                ).astype(jnp.bfloat16)
            at = pl.ds(o * block, block)
            put(stage[3 + n].at[at, :], outputs[3 + n].at[at, :])
    for copy in copies:
        copy.wait()


def body(fs, tp):
    def local(
        mixer_input,
        cell_output,
        query_grad,
        value_grad,
        output_grad,
        query_weight,
        value_weight,
        output_weight,
        query_basis,
        value_basis,
        output_basis,
        query_mean,
        value_mean,
        output_mean,
        query_square,
        value_square,
        output_square,
    ):
        means = (query_mean, value_mean, output_mean)
        olds = (query_square, value_square, output_square)
        weights = (query_weight, value_weight, output_weight)
        w_all, pair, ob, *rest = exchange(
            fs,
            tp,
            mixer_input,
            cell_output,
            (query_grad, value_grad, output_grad),
            (query_basis, value_basis, output_basis),
            weights,
            means,
            olds,
        )
        entries = float(sum(w.shape[0] * fs * w.shape[1] * tp for w in weights))
        pair = pair.reshape(fs, -1, pair.shape[-1])
        ob = ob.reshape(fs, -1, ob.shape[-1])
        f32 = jnp.float32
        shapes = (
            *(jax.ShapeDtypeStruct(w.shape, f32) for w in weights),
            *(jax.ShapeDtypeStruct((w.shape[0] * fs, w.shape[1]), jnp.bfloat16) for w in weights),
            *(jax.ShapeDtypeStruct(m.shape, f32) for m in means),
            *(jax.ShapeDtypeStruct(m.shape, f32) for m in olds),
        )
        vmem = pl.BlockSpec(memory_space=pltpu.VMEM)
        return pl.pallas_call(
            functools.partial(last_kernel, entries),
            out_shape=shapes,
            in_specs=[vmem] * 7,
            out_specs=(pl.BlockSpec(memory_space=pl.ANY),) * 12,
            scratch_shapes=[
                *(pltpu.VMEM(s.shape, s.dtype) for s in shapes[:6]),
                pltpu.SemaphoreType.DMA((9 + 3 * fs,)),
            ],
            compiler_params=pltpu.CompilerParams(vmem_limit_bytes=VMEM_LAST),
        )(w_all, pair, ob, *rest)

    return local


def solution(mesh):
    rows, split_both, columns = P("fs", None), P("fs", "tp"), P(None, "tp")
    in_specs = (rows,) * 2 + (split_both,) * 6 + (rows,) * 3 + (columns,) * 6
    out_specs = (split_both,) * 3 + (columns,) * 9
    return jax.shard_map(
        body(mesh.shape["fs"], mesh.shape["tp"]),
        mesh=mesh,
        in_specs=in_specs,
        out_specs=out_specs,
        check_vma=False,
    )
```

```python
import functools

import jax
import jax.numpy as jnp
from jax import lax
from jax.experimental import pallas as pl
from jax.experimental.pallas import tpu as pltpu
from jax.sharding import PartitionSpec as P

beta_first = 0.8
beta_second = 0.9
floor_mean = 0.005
learn_rate = 0.05

MESH = pl.DeviceIdType.MESH
LINE_SHARE = 8 / 16
BASE_LINES = (0, 1)


def matmul(left, right):
    return jnp.dot(left, right, preferred_element_type=jnp.float32)


def moments(projected, mean_old, square_old):
    moment_one = beta_first * mean_old + (1.0 - beta_first) * projected
    moment_two = beta_second * square_old + (1.0 - beta_second) * projected * projected
    return (moment_one, moment_two, moment_one / jnp.sqrt(moment_two))


def aligned(start, size):
    return pl.ds(pl.multiple_of(start, size), size)


ARRIVE = (0, 1, 2, 2, 1, 0, 0, 1, 2, 3, 3, 2, 1)
LEAVE = (0, 1, 2, 3, 4, 5, 4, 6, 7, 8, 8, 7, 6, 9, 10)


class Gather:
    def __init__(self, fs, me, refs, chunks, lines, piece, several, sems):
        self.fs, self.me, self.refs, self.chunks = fs, me, refs, chunks
        self.lines, self.piece, self.several = lines, piece, several
        self.send_sem, self.step_sem, self.last_sem = sems
        self.relayed = fs == 8
        self.place, self.side = me // 2, lax.rem(me, 2)

    def index(self, step, other=False):
        place = lax.rem(self.place + step + 4, 4)
        return place * 2 + (1 - self.side if other else self.side)

    def arrival(self, w, i, role):
        if self.relayed and role < 6:
            return self.step_sem.at[w, ARRIVE[role], i]
        return self.last_sem.at[w, ARRIVE[role] if self.relayed else role]

    def departure(self, w, site):
        return self.send_sem.at[w, LEAVE[site] if self.relayed else site]

    def copy(self, w, i, origin, site, role, target):
        return remote(
            self.piece(w, origin, i),
            self.piece(w, origin, i),
            self.departure(w, site),
            self.arrival(w, i, role),
            fs=target,
        )

    def total(self, w, origin, count, site, role):
        return remote(
            self.several(w, origin, count),
            self.several(w, origin, count),
            self.departure(w, site),
            self.arrival(w, 0, role),
            fs=lax.rem(self.me + 1, self.fs),
        )

    def arrive(self, w, i, origin, role, inside):
        copy = self.copy(w, i, origin, 0, role, lax.rem(self.me + 1, self.fs))
        pl.when(inside)(copy.wait_recv)

    def sites(self, w, i):
        p = self.place
        line = i < self.lines[w]
        cross = self.index(0, True)
        out = {
            0: (self.me, 0, self.index(1), p < 3),
            1: (self.me, 3, self.index(-1), p > 0),
            2: (self.me, 6, cross, None),
            13: (cross, 7, self.index(1), (p < 3) & (line | (p == 0))),
            14: (cross, 10, self.index(-1), (p > 0) & (line | (p == 3))),
        }
        for d in (1, 2):
            out[2 + d] = (self.index(-d), d, self.index(1), (p >= d) & (p < 3))
            out[4 + d] = (self.index(d), 3 + d, self.index(-1), (p + d < 4) & (p > 0))
        for d in (1, 2, 3):
            below, above = p >= d, p + d < 4
            if d == 1:
                below = below & jnp.logical_not(line | (p == 1))
                above = above & jnp.logical_not(line | (p == 2))
            out[6 + d] = (self.index(-d), 6 + d, cross, below)
            out[9 + d] = (self.index(d), 9 + d, cross, above)
        return out

    def direct(self):
        return [(k - 1, lax.rem(self.me + k, self.fs)) for k in range(1, self.fs)]

    def send(self, w, i, wanted, also=None):
        table = self.sites(w, i)
        for site in wanted:
            origin, role, target, inside = table[site]
            copy = self.copy(w, i, origin, site, role, target)
            if also is not None:
                inside = inside & also
            if inside is None:
                copy.start()
            else:
                pl.when(inside)(copy.start)

    def each(self, step, low=0, high=None):
        high = self.chunks if high is None else high

        def chunk(i, carry):
            for w in range(len(self.refs)):
                step(w, i)
            return carry

        if high - low == 1:
            chunk(low, 0)
        elif high > low:
            lax.fori_loop(low, high, chunk, 0)

    def start(self, low=0, high=None):
        def step(w, i):
            if self.relayed:
                self.send(w, i, (0, 1, 2))
            else:
                for number, target in self.direct():
                    self.copy(w, i, self.me, number, number, target).start()

        self.each(step, low, high)

    def relay_out(self, low=0, high=None):
        p = self.place

        def step(w, i):
            self.arrive(w, i, self.index(-1), 0, p >= 2)
            self.send(w, i, (3, 7), p >= 2)
            self.arrive(w, i, self.index(1), 3, p <= 1)
            self.send(w, i, (5, 10), p <= 1)

        if self.relayed:
            self.each(step, low, high)

    def relay_in(self, low=0, high=None):
        p = self.place

        def step(w, i):
            self.arrive(w, i, self.index(-1), 0, p == 1)
            self.send(w, i, (3,), p == 1)
            self.arrive(w, i, self.index(1), 3, p == 2)
            self.send(w, i, (5,), p == 2)

        if self.relayed:
            self.each(step, low, high)

    def relay(self, d, low=0, high=None):
        p = self.place

        def step(w, i):
            self.arrive(w, i, self.index(-d), d - 1, p >= d)
            self.send(w, i, (2 + d, 6 + d) if d < 3 else (6 + d,))
            self.arrive(w, i, self.index(d), 2 + d, p + d < 4)
            self.send(w, i, (4 + d, 9 + d) if d < 3 else (9 + d,))

        if self.relayed:
            self.each(step, low, high)

    def relay_cross(self):
        if not self.relayed:
            return
        for w in range(len(self.refs)):
            self.total(w, self.index(0, True), self.chunks, 0, 6).wait_recv()
        self.each(lambda w, i: self.send(w, i, (13, 14)))

    def finish(self):
        p = self.place
        for w in range(len(self.refs)):
            if not self.relayed:
                for k in range(1, self.fs):
                    source = lax.rem(self.me + self.fs - k, self.fs)
                    self.total(w, source, self.chunks, 0, k - 1).wait_recv()
                continue
            for d in (1, 2, 3):
                below = self.total(w, self.index(-d, True), self.chunks, 0, 6 + d)
                above = self.total(w, self.index(d, True), self.chunks, 0, 9 + d)
                pl.when(p >= d)(below.wait_recv)
                pl.when(p + d < 4)(above.wait_recv)

    def drain(self):
        p = self.place
        for w in range(len(self.refs)):
            if not self.relayed:
                for number, _ in self.direct():
                    self.total(w, self.me, self.chunks, number, 0).wait_send()
                continue
            on_line, rest = self.lines[w], self.chunks - self.lines[w]
            for site, (origin, _, _, inside) in self.sites(w, 0).items():
                waits = [(self.chunks, inside)]
                if site == 7:
                    waits = [(rest, p >= 2)]
                elif site == 10:
                    waits = [(rest, p <= 1)]
                elif site == 13:
                    waits = [(self.chunks, p == 0), (on_line, (p > 0) & (p < 3))]
                elif site == 14:
                    waits = [(self.chunks, p == 3), (on_line, (p > 0) & (p < 3))]
                for count, when in waits:
                    if count == 0:
                        continue
                    copy = self.total(w, origin, count, site, 0)
                    if when is None:
                        copy.wait_send()
                    else:
                        pl.when(when)(copy.wait_send)


def remote(ref_from, ref_to, send, recv, **device):
    return pltpu.make_async_remote_copy(
        src_ref=ref_from,
        dst_ref=ref_to,
        send_sem=send,
        recv_sem=recv,
        device_id=device,
        device_id_type=MESH,
    )


def kernel(
    fs,
    tp,
    owners,
    mixer_hbm,
    cell_hbm,
    qg_hbm,
    vg_hbm,
    og_hbm,
    qb_hbm,
    vb_hbm,
    ob_hbm,
    qw_hbm,
    vw_hbm,
    ow_hbm,
    qm_hbm,
    vm_hbm,
    om_hbm,
    qs_hbm,
    vs_hbm,
    os_hbm,
    w_all,
    pair_all,
    ob_all,
    firsts,
    seconds,
    dirs,
    squares,
    mixer,
    cell,
    qg,
    vg,
    og,
    qw,
    vw,
    ow,
    means,
    olds,
    proj,
    part,
    parts,
    square_own,
    square_in,
    w_send,
    w_step,
    w_last,
    b_send,
    b_step,
    b_last,
    y_send,
    y_recv,
    c_send,
    c_recv,
    sum_send,
    sum_recv,
    back_send,
    back_recv,
    over_send,
    tp_send,
    tp_recv,
    local_sem,
):
    me, column = lax.axis_index("fs"), lax.axis_index("tp")
    rank, width = qm_hbm.shape
    far, core = column // 2, lax.rem(column, 2)
    fars = tp // 2
    own_bases = (pair_all.at[me, far, core], ob_all.at[me, far, core])
    pair_rows, ob_rows = pair_all.shape[3], ob_all.shape[3]
    pair_from = aligned(column * pair_rows, pair_rows)
    ob_from = aligned(column * ob_rows, ob_rows)
    loads = [
        pltpu.make_async_copy(source, target, local_sem.at[i])
        for i, (source, target) in enumerate(
            (
                (qb_hbm.at[pair_from, :], pair_all.at[me, far, core, :, pl.ds(0, rank)]),
                (vb_hbm.at[pair_from, :], pair_all.at[me, far, core, :, pl.ds(rank, rank)]),
                (ob_hbm.at[ob_from, :], own_bases[1]),
                (qw_hbm, qw),
                (vw_hbm, vw),
                (ow_hbm, ow),
                (mixer_hbm, mixer),
                (cell_hbm, cell),
                (qg_hbm, qg),
                (vg_hbm, vg),
                (og_hbm, og),
                (qm_hbm, means.at[:, pl.ds(0, width)]),
                (vm_hbm, means.at[:, pl.ds(width, width)]),
                (om_hbm, means.at[:, pl.ds(2 * width, 2 * width)]),
                (qs_hbm, olds.at[:, pl.ds(0, width)]),
                (vs_hbm, olds.at[:, pl.ds(width, width)]),
                (os_hbm, olds.at[:, pl.ds(2 * width, 2 * width)]),
            )
        )
    ]
    for load in loads:
        load.start()

    barrier = pltpu.get_barrier_semaphore()

    def greet(target):
        pl.semaphore_signal(
            barrier, inc=1, device_id={"fs": target}, device_id_type=MESH
        )

    place = me // 2
    for k in range(1, tp):
        pl.semaphore_signal(
            barrier, inc=1, device_id={"tp": lax.rem(column + k, tp)}, device_id_type=MESH
        )
    if fs == 8:
        greet(me + 1 - 2 * lax.rem(me, 2))
        pl.when(place < 3)(lambda: greet(lax.rem(me + 2, fs)))
        pl.when(place > 0)(lambda: greet(lax.rem(me + fs - 2, fs)))
        inner = (place > 0) & (place < 3)
        pl.when(inner)(lambda: pl.semaphore_wait(barrier, tp + 2))
        pl.when(jnp.logical_not(inner))(lambda: pl.semaphore_wait(barrier, tp + 1))
    else:
        for k in range(1, fs):
            greet(lax.rem(me + k, fs))
        pl.semaphore_wait(barrier, fs + tp - 2)

    for load in loads[:3]:
        load.wait()
    bases = (pair_all, ob_all)
    sent = []
    parts_of_bases = Gather(
        fs,
        me,
        bases,
        1,
        BASE_LINES,
        lambda w, origin, i: bases[w].at[origin, far, core],
        lambda w, origin, count: bases[w].at[origin, far, core],
        (b_send, b_step, b_last),
    )
    chunks = w_all.shape[1]
    weights = Gather(
        fs,
        me,
        (w_all,),
        chunks,
        (int(LINE_SHARE * chunks),),
        lambda w, origin, i: w_all.at[origin, i],
        lambda w, origin, count: w_all.at[origin, pl.ds(0, count)],
        (w_send, w_step, w_last),
    )
    parts_of_bases.start()
    for load in loads[3:6]:
        load.wait()
    across, spread = w_all.shape[4], ow.shape[1] // w_all.shape[4]
    for n, own in enumerate((qw, vw)):
        w_all[me, :, n] = own[...].astype(jnp.bfloat16).reshape(chunks, -1, across)
    low_rows = w_all.shape[3] // spread
    for h in range(spread):
        piece = ow[:, h * across : (h + 1) * across].astype(jnp.bfloat16)
        w_all[me, :, 2, h * low_rows : (h + 1) * low_rows, :] = piece.reshape(
            chunks, low_rows, across
        )
    weights.start(0, 1)
    part[...] = jnp.zeros_like(part)
    parts_of_bases.relay(1)
    parts_of_bases.relay_cross()
    weights.start(1, 2)
    parts_of_bases.relay(2)
    weights.start(2, 3)
    parts_of_bases.relay(3)
    weights.start(3)
    parts_of_bases.finish()
    for k in range(1, fars):
        for n, whole in enumerate(bases):
            mine = whole.at[:, far, core]
            copy = remote(
                mine,
                mine,
                y_send.at[n, k - 1],
                y_recv.at[n, k - 1],
                tp=lax.rem(far + k, fars) * 2 + core,
            )
            copy.start()
            sent.append(copy)
    weights.relay_out(0, chunks // 2)
    for k in range(1, fars):
        source = lax.rem(far + fars - k, fars)
        for n, whole in enumerate(bases):
            there = whole.at[:, source, core]
            remote(
                there,
                there,
                y_send.at[n, k - 1],
                y_recv.at[n, k - 1],
                tp=lax.rem(far + k, fars) * 2 + core,
            ).wait_recv()
    for n, whole in enumerate(bases):
        mine = whole.at[:, :, core]
        copy = remote(mine, mine, c_send.at[n], c_recv.at[n], tp=far * 2 + 1 - core)
        copy.start()
        sent.append(copy)
    for load in loads[6:]:
        load.wait()
    for n, whole in enumerate(bases):
        there = whole.at[:, :, 1 - core]
        remote(there, there, c_send.at[n], c_recv.at[n], tp=far * 2 + 1 - core).wait_recv()

    tile = 256

    def project(rows, grad):
        turned = jnp.transpose(rows)
        high = turned.astype(jnp.bfloat16)
        low = (turned - high.astype(jnp.float32)).astype(jnp.bfloat16)
        both = matmul(jnp.concatenate([high, low], axis=0), grad)
        return both[:rank] + both[rank:]

    def flat(ref):
        value = ref[...]
        return value.reshape(-1, value.shape[-1])

    def step(t, carry):
        at = aligned(t * tile, tile)
        rows = matmul(mixer[at, :], flat(pair_all))
        part[:, :width] += project(rows[:, :rank], qg[at, :])
        part[:, width : 2 * width] += project(rows[:, rank:], vg[at, :])
        part[:, 2 * width :] += project(matmul(cell[at, :], flat(ob_all)), og[at, :])
        return carry

    lax.fori_loop(0, mixer.shape[0] // tile, step, 0)

    first_owner = (fs - owners) // 2
    share = rank // owners

    def owns(index):
        return (index >= first_owner) & (index < first_owner + owners)

    def strip_of(index):
        return lax.rem(index - first_owner + fs, owners)

    def strip(index):
        return aligned(strip_of(index) * share, share)

    drains = []
    for k in range(1, fs):
        target = lax.rem(me + k, fs)
        copy = remote(
            part.at[strip(target), :],
            parts.at[k - 1],
            sum_send.at[k - 1],
            sum_recv.at[k - 1],
            fs=target,
        )
        pl.when(owns(target))(copy.start)
        drains.append((copy, owns(target)))

    weights.relay_out(chunks // 2)
    weights.relay_in(0, chunks // 4)

    def gram(ref):
        rows, size = ref.shape[3], ref.shape[4]

        def add(i, total):
            piece = ref[i].reshape(-1, size)
            turned = jnp.transpose(piece.astype(jnp.float32)).astype(jnp.bfloat16)
            return total + matmul(turned, piece)

        return lax.fori_loop(0, ref.shape[0], add, jnp.zeros((size, size), jnp.float32))

    gram_pair = gram(pair_all)
    gram_output = gram(ob_all)

    side = lax.rem(me, 2)
    relayed = weights.relayed
    back = []
    for k in range(1, fs):
        target = lax.rem(me + k, fs)
        mine = proj.at[strip(me), :]
        inside = owns(me)
        if relayed:
            inside = inside & (owns(target) | (lax.rem(target, 2) == side))
        copy = remote(
            mine, mine, back_send.at[k - 1], back_recv.at[strip_of(me)], fs=target
        )
        back.append((copy, inside))
    other = me + 1 - 2 * side if relayed else lax.rem(me + 1, fs)
    returned = []
    for j in range(owners):
        there = proj.at[pl.ds(j * share, share), :]
        source = first_owner + j
        straight = me != source
        if relayed:
            same = side == source % 2
            straight = straight & (owns(me) | same)
        over = remote(there, there, over_send.at[j], back_recv.at[j], fs=other)
        returned.append((over, straight, jnp.logical_not(owns(me)) if relayed else None, source % 2))

    @pl.when(owns(me))
    def _():
        for k in range(1, fs):
            remote(
                part.at[strip(me), :],
                parts.at[k - 1],
                sum_send.at[k - 1],
                sum_recv.at[k - 1],
                fs=lax.rem(me + k, fs),
            ).wait_recv()
        total = part[strip(me), :]
        for k in range(1, fs):
            total = total + parts[k - 1]
        proj[strip(me), :] = total.astype(proj.dtype)

    for copy, inside in back:
        pl.when(inside)(copy.start)

    weights.relay_in(chunks // 4)
    weights.relay(2)
    weights.relay_cross()

    for over, straight, at_end, parity in returned:
        pl.when(straight)(over.wait_recv)
        if relayed:
            pl.when(at_end & (side == parity))(over.start)
    weights.relay(3)
    if relayed:
        for over, straight, at_end, parity in returned:
            pl.when(at_end & (side != parity))(over.wait_recv)

    def norm(basis_gram, left, columns):
        at = pl.ds(left, columns)
        first, second, direction = moments(
            proj[:, at].astype(jnp.float32), means[:, at], olds[:, at]
        )
        firsts[:, at] = first
        seconds[:, at] = second
        high = direction.astype(jnp.bfloat16)
        dirs[:rank, at] = high
        dirs[rank:, at] = (direction - high.astype(jnp.float32)).astype(jnp.bfloat16)
        turned = jnp.dot(
            basis_gram,
            direction,
            precision=lax.Precision.HIGHEST,
            preferred_element_type=jnp.float32,
        )
        lanes = jnp.sum(direction * turned, axis=0, keepdims=True)
        return jnp.sum(lanes, axis=1, keepdims=True)

    partial = (
        norm(gram_pair[:rank, :rank], 0, width)
        + norm(gram_pair[rank:, rank:], width, width)
        + norm(gram_output, 2 * width, 2 * width)
    )
    square_own[...] = jnp.broadcast_to(partial, square_own.shape)
    shares = []
    for k in range(1, tp):
        copy = remote(
            square_own,
            square_in.at[k - 1],
            tp_send.at[k - 1],
            tp_recv.at[k - 1],
            tp=lax.rem(column + k, tp),
        )
        copy.start()
        shares.append(copy)

    for copy in shares:
        copy.wait_recv()
    whole_squares = square_own[...]
    for k in range(1, tp):
        whole_squares = whole_squares + square_in[k - 1]
    squares[...] = whole_squares
    weights.finish()
    for copy in sent + shares:
        copy.wait_send()
    for copy, inside in drains + back:
        pl.when(inside)(copy.wait_send)
    if relayed:
        for over, straight, at_end, parity in returned:
            pl.when(at_end & (side == parity))(over.wait_send)
    parts_of_bases.drain()
    weights.drain()


def exchange(fs, tp, mixer, cell, grads, bases, weights, means, olds):
    rank = means[0].shape[0]
    total = sum(grad.shape[1] for grad in grads)
    owners = min(4, fs)
    bf16, f32 = jnp.bfloat16, jnp.float32
    hbm, vmem = pl.BlockSpec(memory_space=pltpu.HBM), pl.BlockSpec(memory_space=pltpu.VMEM)
    dma = pltpu.SemaphoreType.DMA

    rows, across = weights[0].shape
    chunks = min(16, rows * across // (16 * weights[2].shape[1]))

    def parted(array, columns):
        return jax.ShapeDtypeStruct((fs, tp // 2, 2, array.shape[0] // tp, columns), bf16)

    return pl.pallas_call(
        functools.partial(kernel, fs, tp, owners),
        out_shape=(
            jax.ShapeDtypeStruct((fs, chunks, 3, rows // chunks, across), bf16),
            parted(bases[0], 2 * rank),
            parted(bases[2], rank),
            jax.ShapeDtypeStruct((rank, total), f32),
            jax.ShapeDtypeStruct((rank, total), f32),
            jax.ShapeDtypeStruct((2 * rank, total), bf16),
            jax.ShapeDtypeStruct((8, 128), f32),
        ),
        in_specs=[hbm] * 17,
        out_specs=(vmem,) * 7,
        scratch_shapes=[
            *(pltpu.VMEM(array.shape, bf16) for array in (mixer, cell, *grads)),
            *(pltpu.VMEM(array.shape, f32) for array in weights),
            pltpu.VMEM((rank, total), f32),
            pltpu.VMEM((rank, total), f32),
            pltpu.VMEM((rank, total), bf16),
            pltpu.VMEM((rank, total), f32),
            pltpu.VMEM((fs - 1, rank // owners, total), f32),
            pltpu.VMEM((8, 128), f32),
            pltpu.VMEM((tp - 1, 8, 128), f32),
            dma((1, max(11, fs - 1))),
            dma((1, 3, chunks)),
            dma((1, max(4, fs - 1))),
            dma((2, max(11, fs - 1))),
            dma((2, 3, 1)),
            dma((2, max(4, fs - 1))),
            dma((2, max(1, tp // 2 - 1))),
            dma((2, max(1, tp // 2 - 1))),
            dma((2,)),
            dma((2,)),
            dma((fs - 1,)),
            dma((fs - 1,)),
            dma((fs - 1,)),
            dma((owners,)),
            dma((owners,)),
            dma((tp - 1,)),
            dma((tp - 1,)),
            dma((17,)),
        ],
        compiler_params=pltpu.CompilerParams(
            collective_id=0, has_side_effects=True, vmem_limit_bytes=VMEM_MAIN
        ),
    )(*(pltpu.with_memory_space_constraint(a, pltpu.HBM) for a in (mixer, cell, *grads, *bases, *weights, *means, *olds)))


VMEM_MAIN = 30 * 1024 * 1024
VMEM_LAST = 24 * 1024 * 1024


def last_kernel(entries, *refs):
    w_all, pair, ob, firsts, seconds, dirs, squares = refs[:7]
    outputs, stage, sem = refs[7:19], refs[19:25], refs[25]
    rank, across = pair.shape[2] // 2, w_all.shape[4]
    me = lax.axis_index("fs")
    copies = []

    def put(source, target):
        copy = pltpu.make_async_copy(source, target, sem.at[len(copies)])
        copy.start()
        copies.append(copy)

    cuts, left = [], 0
    for output in outputs[:3]:
        cuts.append((left, output.shape[1]))
        left += output.shape[1]
    for n, cut in enumerate(cuts):
        put(firsts.at[:, pl.ds(*cut)], outputs[6 + n])
        put(seconds.at[:, pl.ds(*cut)], outputs[9 + n])
    factor = 1.0 / jnp.sqrt(squares[0:1, 0:1] / entries + floor_mean)
    scale = -learn_rate * factor
    bases = ((pair, 0), (pair, rank), (ob, 0))
    for n, (cut, (base, low)) in enumerate(zip(cuts, bases)):
        both = dirs[:, pl.ds(*cut)]
        own = base[me, :, low : low + rank]
        stage[n][...] = -factor * matmul(jnp.concatenate([own, own], axis=1), both)
        put(stage[n], outputs[n])
        block = base.shape[1]
        rows = block // w_all.shape[1]
        for o in range(base.shape[0]):
            update = scale * matmul(base[o, :, low : low + rank], both[:rank])
            for h in range(cut[1] // across):
                held = w_all[o, :, n, h * rows : (h + 1) * rows, :].reshape(block, across)
                stage[3 + n][pl.ds(o * block, block), h * across : (h + 1) * across] = (
                    held.astype(jnp.float32) + update[:, h * across : (h + 1) * across]
                ).astype(jnp.bfloat16)
            at = pl.ds(o * block, block)
            put(stage[3 + n].at[at, :], outputs[3 + n].at[at, :])
    for copy in copies:
        copy.wait()


def body(fs, tp):
    def local(
        mixer_input,
        cell_output,
        query_grad,
        value_grad,
        output_grad,
        query_weight,
        value_weight,
        output_weight,
        query_basis,
        value_basis,
        output_basis,
        query_mean,
        value_mean,
        output_mean,
        query_square,
        value_square,
        output_square,
    ):
        means = (query_mean, value_mean, output_mean)
        olds = (query_square, value_square, output_square)
        weights = (query_weight, value_weight, output_weight)
        w_all, pair, ob, *rest = exchange(
            fs,
            tp,
            mixer_input,
            cell_output,
            (query_grad, value_grad, output_grad),
            (query_basis, value_basis, output_basis),
            weights,
            means,
            olds,
        )
        entries = float(sum(w.shape[0] * fs * w.shape[1] * tp for w in weights))
        pair = pair.reshape(fs, -1, pair.shape[-1])
        ob = ob.reshape(fs, -1, ob.shape[-1])
        f32 = jnp.float32
        shapes = (
            *(jax.ShapeDtypeStruct(w.shape, f32) for w in weights),
            *(jax.ShapeDtypeStruct((w.shape[0] * fs, w.shape[1]), jnp.bfloat16) for w in weights),
            *(jax.ShapeDtypeStruct(m.shape, f32) for m in means),
            *(jax.ShapeDtypeStruct(m.shape, f32) for m in olds),
        )
        vmem = pl.BlockSpec(memory_space=pltpu.VMEM)
        return pl.pallas_call(
            functools.partial(last_kernel, entries),
            out_shape=shapes,
            in_specs=[vmem] * 7,
            out_specs=(pl.BlockSpec(memory_space=pl.ANY),) * 12,
            scratch_shapes=[
                *(pltpu.VMEM(s.shape, s.dtype) for s in shapes[:6]),
                pltpu.SemaphoreType.DMA((9 + 3 * fs,)),
            ],
            compiler_params=pltpu.CompilerParams(vmem_limit_bytes=VMEM_LAST),
        )(w_all, pair, ob, *rest)

    return local


def solution(mesh):
    rows, split_both, columns = P("fs", None), P("fs", "tp"), P(None, "tp")
    in_specs = (rows,) * 2 + (split_both,) * 6 + (rows,) * 3 + (columns,) * 6
    out_specs = (split_both,) * 3 + (columns,) * 9
    return jax.shard_map(
        body(mesh.shape["fs"], mesh.shape["tp"]),
        mesh=mesh,
        in_specs=in_specs,
        out_specs=out_specs,
        check_vma=False,
    )
```
